256 devices in a mesh: ep: 64 (over z, y, core), tp: 4 (over x).
Axes of the slice: x: 4, y: 4, z: 8, core: 2. Of those that a mesh axis runs over, the one named last changes fastest.
Arguments:
- tokens: bfloat16 [512, 1024], P('ep'), may hold values from -6 to 6
- ssm_state: float32 [512, 32, 64, 128], P('ep', 'tp'), may hold values from -6 to 6
- conv_x: bfloat16 [512, 3, 2048], P('ep', None, 'tp'), may hold values from -6 to 6
- conv_b: bfloat16 [512, 3, 1024], P('ep', None, 'tp'), may hold values from -6 to 6
- conv_c: bfloat16 [512, 3, 1024], P('ep', None, 'tp'), may hold values from -6 to 6
- w_x: bfloat16 [1024, 2048], P(None, 'tp'), may hold values from -0.1875 to 0.1875
- w_z: bfloat16 [1024, 2048], P(None, 'tp'), may hold values from -0.1875 to 0.1875
- w_b: bfloat16 [1024, 1024], P(None, 'tp'), may hold values from -0.1875 to 0.1875
- w_c: bfloat16 [1024, 1024], P(None, 'tp'), may hold values from -0.1875 to 0.1875
- w_dt: bfloat16 [1024, 32], replicated, may hold values from -0.1875 to 0.1875
- dt_bias: float32 [32], P('tp'), may hold values from -2 to 1
- a_log: float32 [32], P('tp'), may hold values from -3 to 1
- d_skip: float32 [32], P('tp'), may hold values from 0.1 to 1.9
- taps_x: bfloat16 [4, 2048], P(None, 'tp'), may hold values from -3 to 3
- taps_b: bfloat16 [4, 1024], P(None, 'tp'), may hold values from -3 to 3
- taps_c: bfloat16 [4, 1024], P(None, 'tp'), may hold values from -3 to 3
- norm1_gain: float32 [1024], replicated, may hold values from 0.1 to 1.9
- group_gain: float32 [2048], P('tp'), may hold values from 0.1 to 1.9
- w_out: bfloat16 [2048, 1024], P('tp'), may hold values from -0.125 to 0.125
- norm2_gain: float32 [1024], replicated, may hold values from 0.1 to 1.9
- route_ids: int32 [512, 6], P('ep'), may hold values from 0 to 63, all different within a row; in each aligned block of 8 rows (0 to 7, 8 to 15, ...) at most 2 rows name the same one
- route_weights: float32 [512, 6], P('ep'), may hold values from 0.1 to 1
- exp_gate: bfloat16 [64, 1024, 512], P('ep', None, 'tp'), may hold values from -0.1875 to 0.1875
- exp_up: bfloat16 [64, 1024, 512], P('ep', None, 'tp'), may hold values from -0.1875 to 0.1875
- exp_down: bfloat16 [64, 512, 1024], P('ep', 'tp'), may hold values from -0.25 to 0.25
- dense_gate: bfloat16 [1024, 1024], P('ep', 'tp'), may hold values from -0.1875 to 0.1875
- dense_up: bfloat16 [1024, 1024], P('ep', 'tp'), may hold values from -0.1875 to 0.1875
- dense_down: bfloat16 [1024, 1024], P('tp', 'ep'), may hold values from -0.1875 to 0.1875
- branch_gate: bfloat16 [1024], replicated, may hold values from -0.375 to 0.375
Outputs:
- mixed: bfloat16 [512, 1024], P('ep', 'tp')
- state_next: float32 [512, 32, 64, 128], P('ep', 'tp')
- conv_x_next: bfloat16 [512, 3, 2048], P('ep', None, 'tp')
- conv_b_next: bfloat16 [512, 3, 1024], P('ep', None, 'tp')
- conv_c_next: bfloat16 [512, 3, 1024], P('ep', None, 'tp')
The draws below stay inside these ranges and needn't reach their ends.
Inputs may be any that keep to these rules, and one draw needn't show every extreme that they name: `route_ids`: each row names 6 different experts. Among the rows of one device no expert is named by more than 2 rows, a bound that some block reaches.
All inputs are finite; a program needn't handle non-finite values.
Results may differ from the reference program's by a relative error of at most 0.019.
Values may be sent and summed in bfloat16 or wider, within the bound.
A program may use at most 64 MiB of HBM per device.

```python
import math
import jax
import jax.numpy as jnp
import numpy as np
from jax import lax

D = 1024
HEADS = 32
HEAD_DIM = 64
STATE_DIM = 128
CONV_TAPS = 4
EXPERT_FF = 512
DENSE_FF = 1024
TOP_K = 6
SEQ_DEV = 8
INNER = 2048
STATE_COLS = 1024
TOKENS = 512
EXPERTS = 64
CAP = 2
N_EP = 64
N_TP = 4


def steps_of(own_key, dims, pieces, least, top_value):
    level, own = 1.0, jax.random.fold_in(own_key, 6)
    for position, parts in pieces:
        draws = jnp.exp(jax.random.uniform(jax.random.fold_in(own, position), (parts,), jnp.float32, least / len(pieces), top_value / len(pieces)))
        level = level * jnp.repeat(draws, dims[position] // parts).reshape([-1 if axis == position else 1 for axis in range(len(dims))])
    return level


def shared_out(stream_key, own, number, rows, amount, top, most, slope):
    order = jax.random.permutation(stream_key, amount)
    heavy_load, ordinary = shares(amount, rows * top, most, slope, True), shares(amount, rows * top, most, slope, False)
    places = jnp.arange(amount)

    def named(sizes, turn):
        used = int((sizes > 0).sum())
        fixed = max(1, used // 4)
        passed = fixed + (places - fixed + turn * (used - fixed)) % max(1, amount - fixed)
        return jnp.zeros((amount,), jnp.int32).at[order[jnp.where(places < fixed, places, passed)]].set(jnp.asarray(sizes, jnp.int32))

    sizes = jnp.where(number % 4 == 0, named(heavy_load, number // 4), named(ordinary, number - number // 4 - 1))
    mixed = jax.random.permutation(jax.random.fold_in(own, 3), amount)
    source_of, receiver = mixed[0:amount // 2 * 2:2], mixed[1:amount // 2 * 2:2]
    margin = jnp.minimum(sizes[source_of] - 1, most - sizes[receiver]) // 2
    margin = jnp.where((source_of == order[0]) | (receiver == order[0]) | (sizes[receiver] == 0), 0, jnp.maximum(margin, 0))
    passed = jax.random.randint(jax.random.fold_in(own, 4), (amount // 2,), 0, 1 << 20) % (margin + 1)
    sizes = sizes.at[source_of].add(-passed).at[receiver].add(passed)
    items = jnp.searchsorted(jnp.cumsum(sizes), jnp.arange(rows * top), side="right").astype(jnp.int32)
    table = items.reshape(top, rows).T
    table = table[jax.random.permutation(jax.random.fold_in(own, 1), rows)]
    turn = jax.random.randint(jax.random.fold_in(own, 2), (rows, 1), 0, top)
    return jnp.take_along_axis(table, (jnp.arange(top)[None, :] + turn) % top, axis=1)


def shares(count, total, bound, slope, full):
    loads = [(1 << 20) // math.isqrt(standing ** slope) + 1 for standing in range(1, count + 1)]
    largest = bound if full else min(bound, max(-(-total // count), total * loads[0] // sum(loads)))
    least = 1 if total - largest >= count - 1 else 0
    holding, surplus = [largest] + [least] * (count - 1), total - largest - least * (count - 1)
    while surplus > 0:
        candidates = [i for i in range(1, count) if holding[i] < largest] or [i for i in range(1, count) if holding[i] < bound]
        mass, left = sum([loads[i] for i in candidates]), surplus
        for i in candidates:
            extra = min(bound - holding[i], max(1, left * loads[i] // mass), surplus)
            holding[i] = holding[i] + extra
            surplus = surplus - extra
    return np.array(holding)


def scatter_about(own_key, shape, scale, most, pieces=(), kind=jnp.bfloat16):
    drawn = jax.random.normal(own_key, shape, jnp.float32) * scale
    if len(pieces) > 0:
        drawn = steps_of(own_key, shape, pieces, -0.22, 0.18) * drawn
    return jnp.clip(drawn, min=-most, max=most).astype(kind)


def setup_inputs(seed: int = 0) -> dict:
    keys = jax.random.split(jax.random.key(seed), 30)
    tokens = scatter_about(keys[0], (TOKENS, D), 1.0, 6.0, ((0, 64),))
    ssm_state = scatter_about(keys[1], (TOKENS, HEADS, HEAD_DIM, STATE_DIM), 1.0, 6.0, ((0, 64), (1, 4)), jnp.float32)
    conv_x = scatter_about(keys[2], (TOKENS, CONV_TAPS - 1, INNER), 1.0, 6.0, ((0, 64), (2, 4)))
    conv_b = scatter_about(keys[3], (TOKENS, CONV_TAPS - 1, STATE_COLS), 1.0, 6.0, ((0, 64), (2, 4)))
    conv_c = scatter_about(keys[4], (TOKENS, CONV_TAPS - 1, STATE_COLS), 1.0, 6.0, ((0, 64), (2, 4)))
    w_x = scatter_about(keys[5], (D, INNER), D ** -0.5, 0.1875, ((1, 4),))
    w_z = scatter_about(keys[6], (D, INNER), D ** -0.5, 0.1875, ((1, 4),))
    w_b = scatter_about(keys[7], (D, STATE_COLS), D ** -0.5, 0.1875, ((1, 4),))
    w_c = scatter_about(keys[8], (D, STATE_COLS), D ** -0.5, 0.1875, ((1, 4),))
    w_dt = scatter_about(keys[9], (D, HEADS), D ** -0.5, 0.1875)
    dt_bias = jnp.clip(-2.0 + 3.0 * jax.random.uniform(keys[10], (HEADS,), jnp.float32) ** steps_of(keys[10], (HEADS,), ((0, 4),), -0.2, 0.2), -2.0, 1.0)
    a_log = jnp.clip(-3.0 + 4.0 * jax.random.uniform(keys[11], (HEADS,), jnp.float32) ** steps_of(keys[11], (HEADS,), ((0, 4),), -0.2, 0.2), -3.0, 1.0)
    d_skip = jnp.clip(1.0 + 0.18 * jax.random.normal(keys[12], (HEADS,), jnp.float32), 0.1, 1.9)
    taps_x = scatter_about(keys[13], (CONV_TAPS, INNER), CONV_TAPS ** -0.5, 3.0, ((1, 4),))
    taps_b = scatter_about(keys[14], (CONV_TAPS, STATE_COLS), CONV_TAPS ** -0.5, 3.0, ((1, 4),))
    taps_c = scatter_about(keys[15], (CONV_TAPS, STATE_COLS), CONV_TAPS ** -0.5, 3.0, ((1, 4),))
    norm1_gain = jnp.clip(1.0 + 0.18 * jax.random.normal(keys[16], (D,), jnp.float32), 0.1, 1.9)
    group_gain = jnp.clip(1.0 + 0.18 * jax.random.normal(keys[17], (INNER,), jnp.float32), 0.1, 1.9)
    w_out = scatter_about(keys[18], (INNER, D), INNER ** -0.5, 0.125, ((0, 4),))
    norm2_gain = jnp.clip(1.0 + 0.18 * jax.random.normal(keys[19], (D,), jnp.float32), 0.1, 1.9)
    route_ids_keys = jax.random.split(jax.random.fold_in(keys[20], 1), TOKENS // SEQ_DEV)
    route_ids_turns = jax.random.permutation(jax.random.fold_in(keys[20], 3), TOKENS // SEQ_DEV)
    route_ids = jax.vmap(lambda own, number: shared_out(jax.random.fold_in(keys[20], 2), own, number, SEQ_DEV, EXPERTS, TOP_K, CAP, 2))(route_ids_keys, route_ids_turns).reshape((TOKENS, TOP_K))
    route_weights = jnp.clip(0.1 + 0.9 * jax.random.uniform(keys[21], (TOKENS, TOP_K), jnp.float32) ** steps_of(keys[21], (TOKENS, TOP_K), ((0, 64),), -0.2, 0.2), 0.1, 1.0)
    exp_gate = scatter_about(keys[22], (EXPERTS, D, EXPERT_FF), D ** -0.5, 0.1875, ((0, 64), (2, 4)))
    exp_up = scatter_about(keys[23], (EXPERTS, D, EXPERT_FF), D ** -0.5, 0.1875, ((0, 64), (2, 4)))
    exp_down = scatter_about(keys[24], (EXPERTS, EXPERT_FF, D), EXPERT_FF ** -0.5, 0.25, ((0, 64), (1, 4)))
    dense_gate = scatter_about(keys[25], (D, DENSE_FF), D ** -0.5, 0.1875, ((0, 64), (1, 4)))
    dense_up = scatter_about(keys[26], (D, DENSE_FF), D ** -0.5, 0.1875, ((0, 64), (1, 4)))
    dense_down = scatter_about(keys[27], (DENSE_FF, D), DENSE_FF ** -0.5, 0.1875, ((0, 4), (1, 64)))
    branch_gate = scatter_about(keys[28], (D,), (D // 4) ** -0.5, 0.375)
    return dict(tokens=tokens, ssm_state=ssm_state, conv_x=conv_x, conv_b=conv_b, conv_c=conv_c, w_x=w_x, w_z=w_z, w_b=w_b, w_c=w_c, w_dt=w_dt, dt_bias=dt_bias, a_log=a_log, d_skip=d_skip, taps_x=taps_x, taps_b=taps_b, taps_c=taps_c, norm1_gain=norm1_gain, group_gain=group_gain, w_out=w_out, norm2_gain=norm2_gain, route_ids=route_ids, route_weights=route_weights, exp_gate=exp_gate, exp_up=exp_up, exp_down=exp_down, dense_gate=dense_gate, dense_up=dense_up, dense_down=dense_down, branch_gate=branch_gate)


epsilon = 1e-06

def rms_rows(values, gain):
    return values * lax.rsqrt(lax.optimization_barrier(jnp.mean(values * values, axis=-1, keepdims=True)) + epsilon) * gain

def blocked_sum(left, right, blocks):
    width = left.shape[1] // blocks
    total = jnp.zeros((left.shape[0], right.shape[1]), jnp.float32)
    for index in range(blocks):
        partial_term = jnp.dot(left[:, index * width:(index + 1) * width], right[index * width:(index + 1) * width], preferred_element_type=jnp.float32)
        rounded = lax.optimization_barrier(partial_term.astype(jnp.bfloat16))
        total = total + rounded.astype(jnp.float32)
    return total

def short_conv(previous, fresh, taps):
    window = jnp.concatenate((previous, fresh[:, None]), axis=1)
    summed = lax.optimization_barrier(jnp.sum(window.astype(jnp.float32) * taps.astype(jnp.float32)[None], axis=1))
    return (jax.nn.silu(summed), window[:, 1:])

def mixer_core(x_new, z_new, b_new, c_new, dt_raw, ssm_state, conv_x, conv_b, conv_c, dt_bias, a_log, d_skip, taps_x, taps_b, taps_c, group_gain):
    seqs, heads, head_dim, state_dim = ssm_state.shape
    groups = b_new.shape[1] // state_dim
    x_conv, conv_x_next = short_conv(conv_x, x_new, taps_x)
    b_conv, conv_b_next = short_conv(conv_b, b_new, taps_b)
    c_conv, conv_c_next = short_conv(conv_c, c_new, taps_c)
    x_heads = x_conv.reshape(seqs, heads, head_dim)
    b_heads = jnp.repeat(b_conv.reshape(seqs, groups, state_dim), heads // groups, axis=1)
    c_heads = jnp.repeat(c_conv.reshape(seqs, groups, state_dim), heads // groups, axis=1)
    step = jax.nn.softplus(dt_raw + dt_bias)
    decay = jnp.exp(-step * jnp.exp(a_log))
    state_next = decay[:, :, None, None] * ssm_state + (step[:, :, None] * x_heads)[:, :, :, None] * b_heads[:, :, None, :]
    readout = jnp.einsum('shpn,shn->shp', state_next, c_heads, precision=lax.Precision.HIGHEST) + d_skip[None, :, None] * x_heads
    gated = readout.reshape(seqs, heads * head_dim) * jax.nn.silu(z_new.astype(jnp.float32))
    grouped = gated.reshape(seqs, groups, -1)
    grouped = grouped * lax.rsqrt(lax.optimization_barrier(jnp.mean(grouped * grouped, axis=-1, keepdims=True)) + epsilon)
    mixed_heads = (grouped.reshape(seqs, heads * head_dim) * group_gain).astype(jnp.bfloat16)
    return (mixed_heads, state_next, conv_x_next, conv_b_next, conv_c_next)

def reference(tokens, ssm_state, conv_x, conv_b, conv_c, w_x, w_z, w_b, w_c, w_dt, dt_bias, a_log, d_skip, taps_x, taps_b, taps_c, norm1_gain, group_gain, w_out, norm2_gain, route_ids, route_weights, exp_gate, exp_up, exp_down, dense_gate, dense_up, dense_down, branch_gate):
    stream = tokens.astype(jnp.float32)
    normed = rms_rows(stream, norm1_gain).astype(jnp.bfloat16)
    x_new = jnp.dot(normed, w_x, preferred_element_type=jnp.float32).astype(jnp.bfloat16)
    z_new = jnp.dot(normed, w_z, preferred_element_type=jnp.float32).astype(jnp.bfloat16)
    b_new = jnp.dot(normed, w_b, preferred_element_type=jnp.float32).astype(jnp.bfloat16)
    c_new = jnp.dot(normed, w_c, preferred_element_type=jnp.float32).astype(jnp.bfloat16)
    dt_raw = jnp.dot(normed, w_dt, preferred_element_type=jnp.float32)
    mixed_heads, state_next, conv_x_next, conv_b_next, conv_c_next = mixer_core(x_new, z_new, b_new, c_new, dt_raw, ssm_state, conv_x, conv_b, conv_c, dt_bias, a_log, d_skip, taps_x, taps_b, taps_c, group_gain)
    residual = (stream + blocked_sum(mixed_heads, w_out, N_TP)).astype(jnp.bfloat16)
    normed2 = rms_rows(residual.astype(jnp.float32), norm2_gain).astype(jnp.bfloat16)
    expert_iota = jnp.arange(EXPERTS, dtype=jnp.int32)
    matches = route_ids[:, :, None] == expert_iota[None, None, :]
    routed = lax.optimization_barrier(jnp.sum(matches.astype(jnp.int32), axis=1))
    weight_of = lax.optimization_barrier(jnp.sum(jnp.where(matches, route_weights[:, :, None], jnp.float32(0.0)), axis=1))
    blocked = routed.reshape(N_EP, SEQ_DEV, EXPERTS)
    ranked = (jnp.cumsum(blocked, axis=1) - blocked).reshape(TOKENS, EXPERTS)
    token_iota = jnp.arange(TOKENS, dtype=jnp.int32)
    source = token_iota // SEQ_DEV
    total_slots = EXPERTS * N_EP * CAP
    target = expert_iota[None, :] * (N_EP * CAP) + source[:, None] * CAP + ranked
    target = jnp.where(routed > 0, target, total_slots).astype(jnp.int32)
    owners = jnp.broadcast_to(token_iota[:, None], (TOKENS, EXPERTS)).reshape(-1)
    slot_token = jnp.zeros((total_slots,), jnp.int32).at[target.reshape(-1)].set(owners, mode='drop')
    slot_weight = jnp.zeros((total_slots,), jnp.float32).at[target.reshape(-1)].set(weight_of.reshape(-1), mode='drop')

    def run_expert(operands):
        index_rows, gate_weight, up_weight, down_weight = operands
        chosen = normed2[index_rows]
        gate_pre = jnp.dot(chosen, gate_weight, preferred_element_type=jnp.float32)
        up_pre = jnp.dot(chosen, up_weight, preferred_element_type=jnp.float32)
        active = (jax.nn.silu(gate_pre) * up_pre).astype(jnp.bfloat16)
        return blocked_sum(active, down_weight, N_TP).astype(jnp.bfloat16)
    slot_out = lax.map(run_expert, (slot_token.reshape(EXPERTS, N_EP * CAP), exp_gate, exp_up, exp_down))
    expert_sum = jnp.zeros((TOKENS, D), jnp.float32).at[slot_token].add(slot_weight[:, None] * slot_out.reshape(total_slots, D).astype(jnp.float32))
    dense_pre = jnp.dot(normed2, dense_gate, preferred_element_type=jnp.float32)
    dense_lift = jnp.dot(normed2, dense_up, preferred_element_type=jnp.float32)
    dense_active = (jax.nn.silu(dense_pre) * dense_lift).astype(jnp.bfloat16)
    dense_out = blocked_sum(dense_active, dense_down, N_TP)
    branch = jax.nn.sigmoid(jnp.dot(normed2, branch_gate[:, None], preferred_element_type=jnp.float32))
    mixed = (residual.astype(jnp.float32) + expert_sum + branch * dense_out).astype(jnp.bfloat16)
    return (mixed, state_next, conv_x_next, conv_b_next, conv_c_next)
```

```python
import functools

import jax
import jax.numpy as jnp
from jax import lax
from jax.experimental import pallas as pl
from jax.experimental.pallas import tpu as pltpu
from jax.sharding import PartitionSpec as P

EPS = 1e-06
F32 = jnp.float32
BF16 = jnp.bfloat16
HIGH = lax.Precision.HIGHEST
MESH = pl.DeviceIdType.MESH


def dot(a, b, **kw):
    return jnp.dot(a, b, preferred_element_type=F32, **kw)


def dot_nt(a, b, **kw):
    return lax.dot_general(a, b, (((1,), (1,)), ((), ())), preferred_element_type=F32, **kw)


def iota(shape, dim):
    return lax.broadcasted_iota(jnp.int32, shape, dim)


def rms_rows(values, gain):
    return values * lax.rsqrt(jnp.mean(values * values, axis=-1, keepdims=True) + EPS) * gain


def silu(v):
    return v * jax.nn.sigmoid(v)


def mixer_kernel(
    tokens, state, conv_x, conv_b, conv_c, w_x, w_z, w_b, w_c, w_dt, dt_bias, a_log, d_skip, taps_x, taps_b, taps_c, gain,
    state_out, cx_out, cb_out, cc_out, y_out, z_out,
    st, vx, vz, vb, vc, wsem, isem, osem,
):
    seqs, heads, hd, sd = state.shape
    per = heads * sd // vb.shape[1]
    groups = heads // per
    loads = [pltpu.make_async_copy(src, dst, wsem.at[i]) for i, (src, dst) in enumerate(((w_x, vx), (w_b, vb), (w_c, vc), (w_z, vz)))]
    for c in loads:
        c.start()
    ins = [pltpu.make_async_copy(state.at[s], st.at[s], isem.at[s]) for s in range(seqs)]
    for c in ins:
        c.start()
    normed = rms_rows(tokens[...].astype(F32), gain[...]).astype(BF16)
    width = heads * hd
    me = lax.axis_index("tp")
    raw = dot_nt(normed, w_dt[...])
    all_heads = raw.shape[1]
    spread_all = (iota((all_heads, width), 0) == me * heads + iota((all_heads, width), 1) // hd).astype(F32)
    spread = (iota((heads, width), 0) == iota((heads, width), 1) // hd).astype(F32)
    raw = dot(raw, spread_all, precision=HIGH)
    bias = dot(dt_bias[...], spread, precision=HIGH)
    rate = jnp.exp(dot(a_log[...], spread, precision=HIGH))
    skip = dot(d_skip[...], spread, precision=HIGH)
    pre = raw + bias
    step = jnp.maximum(pre, 0.0) + jnp.log1p(jnp.exp(-jnp.abs(pre)))
    decay = jnp.exp(-step * rate)

    def conv(prev, fresh, taps, out):
        fresh = fresh.astype(BF16)
        tap = taps[...].astype(F32)
        depth = prev.shape[0]
        total = fresh.astype(F32) * tap[depth : depth + 1]
        for j in range(depth):
            total = total + prev[j].astype(F32) * tap[j : j + 1]
            out[j] = prev[j + 1] if j + 1 < depth else fresh
        return silu(total)

    loads[0].wait()
    xs = conv(conv_x, dot(normed, vx[...]), taps_x, cx_out)
    loads[1].wait()
    bs = conv(conv_b, dot(normed, vb[...]), taps_b, cb_out)
    loads[2].wait()
    cs = conv(conv_c, dot(normed, vc[...]), taps_c, cc_out)
    loads[3].wait()
    z_out[...] = dot(normed, vz[...]).astype(BF16).astype(F32)
    in_col = (step * xs).T
    decay_col = decay.T
    rows = per * hd
    lane = iota((rows, seqs), 1)
    reads = [jnp.zeros((rows, seqs), F32) for _ in range(groups)]
    outs = []
    for s in range(seqs):
        ins[s].wait()
        for g in range(groups):
            cut = slice(g * rows, (g + 1) * rows)
            old = st[s, g * per : (g + 1) * per].reshape(rows, sd)
            new = decay_col[cut, s : s + 1] * old + in_col[cut, s : s + 1] * bs[s : s + 1, g * sd : (g + 1) * sd]
            st[s, g * per : (g + 1) * per] = new.reshape(per, hd, sd)
            got = jnp.sum(new * cs[s : s + 1, g * sd : (g + 1) * sd], axis=1, keepdims=True)
            reads[g] = jnp.where(lane == s, got, reads[g])
        c = pltpu.make_async_copy(st.at[s], state_out.at[s], osem.at[s])
        c.start()
        outs.append(c)
    y_out[...] = jnp.concatenate(reads, axis=0).T + skip * xs
    for c in outs:
        c.wait()


PHASES = ("dense", "route", "part", "tok", "slot", "pre", "act", "exp", "dout", "ret", "comb")


def branch_kernel(
    NZ, NC, NT, n_groups,
    tokens, y_in, z_in, ggain, w_out, gain2, ids, wts, w_g, w_u, w_d, dgate, dup, ddown, bgate,
    mixed,
    vo, vg, vu, vd,
    dw, rt, pt, tk, bs_, br, cs_, cr, ac, xs_, xr, fs_, fr, gs_, gr, hs_, hr,
    ssem, rsem, lsem,
):
    S, D = tokens.shape
    inner = y_in.shape[1]
    quarter = D // NT
    planes = NZ // NT
    slots = 2 * NC
    E = NZ * NC
    e = lax.axis_index("ep")
    t = lax.axis_index("tp")
    z = e // NC
    yc = lax.rem(e, NC)
    q_mine = z // planes
    f_self = q_mine == t

    loads = [pltpu.make_async_copy(src, dst, lsem.at[i]) for i, (src, dst) in enumerate(((w_out, vo), (w_g.at[0], vg), (w_u.at[0], vu), (w_d.at[0], vd)))]
    for c in loads:
        c.start()

    zs = [lax.rem(z + d, NZ) for d in range(1, NZ)]
    cores = [lax.rem(yc + d, NC) for d in range(1, NC)]
    ts = [lax.rem(t + d, NT) for d in range(1, NT)]
    barrier = pltpu.get_barrier_semaphore()

    def greet(dev):
        pl.semaphore_signal(barrier, inc=1, device_id=dev, device_id_type=MESH)

    for p in zs:
        greet((p * NC + yc, t))
    for p in cores:
        greet((z * NC + p, t))
    for p in ts:
        greet((e, p))
    for a in range(planes):
        for b in range(NT):
            other_z = t * planes + a

            @pl.when(jnp.logical_or(other_z != z, b != t))
            def _():
                greet((other_z * NC + yc, b))

    sent = []

    def send(phase, src, dst, dev, slot):
        i = PHASES.index(phase)
        c = pltpu.make_async_remote_copy(
            src_ref=src, dst_ref=dst, send_sem=ssem.at[i, len([1 for s in sent if s[0] == i])], recv_sem=rsem.at[i, slot], device_id=dev, device_id_type=MESH
        )
        c.start()
        sent.append((i, c))

    def arrive(phase, ref, slot):
        i = PHASES.index(phase)
        pltpu.make_async_copy(ref.at[slot], ref.at[slot], rsem.at[i, slot]).wait()

    dw[yc] = jnp.concatenate([dgate[...].astype(F32), dup[...].astype(F32), ddown[...].astype(F32)], axis=1).astype(BF16)
    lane = iota((S, 2 * E), 1)
    named = jnp.zeros((S, 2 * E), F32)
    weight = jnp.zeros((S, 2 * E), F32)
    for k in range(ids.shape[1]):
        hit = ids[:, k : k + 1] == lane // 2
        named = jnp.where(hit, 1.0, named)
        weight = jnp.where(hit, wts[:, k : k + 1], weight)
    before = (iota((S, S), 0) > iota((S, S), 1)).astype(F32)
    rank = dot(before, named)
    mine = jnp.logical_and(named > 0.5, jnp.abs(rank - lax.rem(lane, 2).astype(F32)) < 0.5)
    rt[z] = jnp.concatenate([jnp.where(mine, 1.0, 0.0), jnp.where(mine, weight, 0.0)], axis=1).astype(BF16)

    gated = y_in[...] * silu(z_in[...])
    width = inner // n_groups
    parts = []
    for g in range(inner // width):
        v = gated[:, g * width : (g + 1) * width]
        parts.append(v * lax.rsqrt(jnp.mean(v * v, axis=-1, keepdims=True) + EPS) * ggain[:, g * width : (g + 1) * width])
    heads = jnp.concatenate(parts, axis=1).astype(BF16)
    loads[0].wait()
    pt[t] = dot(heads, vo[...]).astype(BF16)

    n_wait = (NZ - 1) + (NC - 1) + (NT - 1) + NZ
    pl.semaphore_wait(barrier, n_wait - f_self.astype(jnp.int32))

    for p in ts:
        send("part", pt.at[t], pt.at[t], (e, p), t)
    for p in zs:
        send("route", rt.at[z], rt.at[z], (p * NC + yc, t), z)
    for p in cores:
        send("dense", dw.at[yc], dw.at[yc], (z * NC + p, t), yc)

    for p in ts:
        arrive("part", pt, p)
    total = pt[0].astype(F32)
    for k in range(1, NT):
        total = total + pt[k].astype(F32)
    residual = (tokens[...].astype(F32) + total).astype(BF16).astype(F32)
    normed = rms_rows(residual, gain2[...]).astype(BF16)
    tk[z] = normed
    for p in zs:
        send("tok", tk.at[z], tk.at[z], (p * NC + yc, t), z)
    lanes = bgate.shape[1]
    weighted = jnp.zeros((S, lanes), F32)
    for k in range(bgate.shape[0]):
        weighted = weighted + normed[:, k * lanes : (k + 1) * lanes].astype(F32) * bgate[k : k + 1, :].astype(F32)
    branch = jax.nn.sigmoid(jnp.sum(weighted, axis=1, keepdims=True))
    own = jnp.zeros((S, quarter), F32)
    for k in range(NT):
        own = jnp.where(t == k, residual[:, k * quarter : (k + 1) * quarter], own)

    for p in zs:
        arrive("route", rt, p)
    routes = jnp.concatenate([rt[k].astype(F32) for k in range(NZ)], axis=0)
    R = NC * NZ * 2
    row, col = iota((R, 2 * E), 0), iota((R, 2 * E), 1)
    pick = (col == z * slots + 2 * (row // (2 * NZ)) + lax.rem(row, 2)).astype(BF16)
    same = lax.rem(iota((R, NZ * S), 0) // 2, NZ) == iota((R, NZ * S), 1) // S
    take = jnp.where(same, dot_nt(pick, routes[:, : 2 * E].astype(BF16)), 0.0).astype(BF16)
    same_t = lax.rem(iota((NZ * S, R), 1) // 2, NZ) == iota((NZ * S, R), 0) // S
    give = jnp.where(same_t, dot_nt(routes[:, 2 * E :].astype(BF16), pick), 0.0).astype(BF16)

    for p in zs:
        arrive("tok", tk, p)
    toks = jnp.concatenate([tk[k].astype(F32) for k in range(NZ)], axis=0).astype(BF16)
    bs_[...] = dot(take, toks).astype(BF16).reshape(bs_.shape)
    for p in cores:
        send("slot", bs_.at[p], br.at[yc], (z * NC + p, t), yc)
    br[yc] = bs_[yc]

    for p in cores:
        arrive("dense", dw, p)
    depth = D // NZ
    cut = pl.ds(pl.multiple_of(z * depth, depth), depth)
    mine_cols = jnp.concatenate([tk[k, :, cut].astype(F32) for k in range(NZ)], axis=0).astype(BF16)
    hid = dw.shape[2] // 3
    plane_w = jnp.concatenate([dw[k] for k in range(NC)], axis=0)
    cs_[...] = dot(mine_cols, plane_w[:, : 2 * hid]).astype(BF16).astype(F32).reshape(NZ, S, 2 * hid).astype(BF16)
    for p in zs:
        send("pre", cs_.at[p], cr.at[z], (p * NC + yc, t), z)
    cr[z] = cs_[z]
    for p in zs:
        arrive("pre", cr, p)
    pre = cr[0].astype(F32)
    for k in range(1, NZ):
        pre = pre + cr[k].astype(F32)
    ac[z] = (silu(pre[:, :hid]) * pre[:, hid:]).astype(BF16)
    for p in zs:
        send("act", ac.at[z], ac.at[z], (p * NC + yc, t), z)

    for c in loads[1:]:
        c.wait()
    for p in cores:
        arrive("slot", br, p)
    rows_in = br[...].reshape(R, D)
    active = (silu(dot(rows_in, vg[...])) * dot(rows_in, vu[...])).astype(BF16)
    for k in range(NT):
        xs_[k] = dot(active, vd[:, k * quarter : (k + 1) * quarter]).astype(BF16)
    for p in ts:
        send("exp", xs_.at[p], xr.at[t], (e, p), t)
    xr[t] = xs_[t]

    for p in zs:
        arrive("act", ac, p)
    acts = jnp.concatenate([ac[k].astype(F32) for k in range(NZ)], axis=0).astype(BF16)
    fs_[...] = dot_nt(acts, plane_w[:, 2 * hid :]).reshape(fs_.shape).astype(BF16)
    f_slot = lax.rem(z, planes) * NT + t
    i = PHASES.index("dout")
    f_copies = []
    for k in range(NZ):
        there = jnp.logical_or(z != k, jnp.logical_not(f_self))
        c = pltpu.make_async_remote_copy(
            src_ref=fs_.at[k], dst_ref=fr.at[f_slot], send_sem=ssem.at[i, k], recv_sem=rsem.at[i, f_slot], device_id=(k * NC + yc, q_mine), device_id_type=MESH
        )
        f_copies.append((there, c))

        @pl.when(there)
        def _():
            c.start()

    @pl.when(f_self)
    def _():
        fr[f_slot] = fs_[z]

    for p in ts:
        arrive("exp", xr, p)
    summed = xr[0].astype(F32)
    for k in range(1, NT):
        summed = summed + xr[k].astype(F32)
    gs_[...] = summed.astype(BF16).reshape(gs_.shape)
    for p in cores:
        send("ret", gs_.at[p], gr.at[yc], (z * NC + p, t), yc)
    gr[yc] = gs_[yc]
    for p in cores:
        arrive("ret", gr, p)
    hs_[...] = dot(give, gr[...].reshape(R, quarter)).reshape(hs_.shape).astype(BF16)
    for p in zs:
        send("comb", hs_.at[p], hr.at[z], (p * NC + yc, t), z)
    hr[z] = hs_[z]

    for a in range(planes):
        for b in range(NT):
            slot = a * NT + b

            @pl.when(jnp.logical_or(t * planes + a != z, b != t))
            def _():
                arrive("dout", fr, slot)

    dense = []
    for a in range(planes):
        v = fr[a * NT].astype(F32)
        for b in range(1, NT):
            v = v + fr[a * NT + b].astype(F32)
        dense.append(v)
    dense = jnp.concatenate(dense, axis=1)
    for p in zs:
        arrive("comb", hr, p)
    expert = hr[0].astype(F32)
    for k in range(1, NZ):
        expert = expert + hr[k].astype(F32)
    mixed[...] = (own + expert + branch * dense).astype(BF16)
    for _, c in sent:
        c.wait_send()
    for there, c in f_copies:

        @pl.when(there)
        def _():
            c.wait_send()


def body(
    tokens, ssm_state, conv_x, conv_b, conv_c, w_x, w_z, w_b, w_c, w_dt, dt_bias, a_log, d_skip, taps_x, taps_b, taps_c,
    norm1_gain, group_gain, w_out, norm2_gain, route_ids, route_weights, exp_gate, exp_up, exp_down, dense_gate, dense_up, dense_down, branch_gate,
    *, NZ, NC, NT, sd,
):
    S, D = tokens.shape
    heads, hd = ssm_state.shape[1:3]
    inner = w_x.shape[1]
    cols = w_b.shape[1]
    vm, hbm = pl.BlockSpec(memory_space=pltpu.VMEM), pl.BlockSpec(memory_space=pl.ANY)
    dma = pltpu.SemaphoreType.DMA
    state_next, cx, cb, cc, y, zz = pl.pallas_call(
        mixer_kernel,
        name="mixer",
        out_shape=(
            jax.ShapeDtypeStruct(ssm_state.shape, F32),
            jax.ShapeDtypeStruct((3, S, inner), BF16),
            jax.ShapeDtypeStruct((3, S, cols), BF16),
            jax.ShapeDtypeStruct((3, S, cols), BF16),
            jax.ShapeDtypeStruct((S, inner), F32),
            jax.ShapeDtypeStruct((S, inner), F32),
        ),
        in_specs=[vm, hbm, vm, vm, vm, hbm, hbm, hbm, hbm] + [vm] * 8,
        out_specs=(hbm, vm, vm, vm, vm, vm),
        scratch_shapes=[
            pltpu.VMEM(ssm_state.shape, F32),
            pltpu.VMEM((D, inner), BF16),
            pltpu.VMEM((D, inner), BF16),
            pltpu.VMEM((D, cols), BF16),
            pltpu.VMEM((D, cols), BF16),
            dma((4,)),
            dma((S,)),
            dma((S,)),
        ],
        compiler_params=pltpu.CompilerParams(vmem_limit_bytes=60_000_000),
    )(
        tokens, ssm_state, turned(conv_x), turned(conv_b), turned(conv_c), w_x, w_z, w_b, w_c, w_dt.T, dt_bias[None], a_log[None], d_skip[None], taps_x, taps_b, taps_c, norm1_gain[None]
    )
    quarter = D // NT
    hidden, dhid = exp_gate.shape[2], dense_gate.shape[1]
    R = NZ * NC * 2
    mixed = pl.pallas_call(
        functools.partial(branch_kernel, NZ, NC, NT, cols // sd),
        name="branches",
        out_shape=jax.ShapeDtypeStruct((S, quarter), BF16),
        in_specs=[vm, vm, vm, vm, hbm, vm, vm, vm, hbm, hbm, hbm, vm, vm, vm, vm],
        out_specs=vm,
        scratch_shapes=[
            pltpu.VMEM((inner, D), BF16),
            pltpu.VMEM((D, hidden), BF16),
            pltpu.VMEM((D, hidden), BF16),
            pltpu.VMEM((hidden, D), BF16),
            pltpu.VMEM((NC, dense_gate.shape[0], 3 * dhid), BF16),
            pltpu.VMEM((NZ, S, 4 * NZ * NC), BF16),
            pltpu.VMEM((NT, S, D), BF16),
            pltpu.VMEM((NZ, S, D), BF16),
            pltpu.VMEM((NC, 2 * NZ, D), BF16),
            pltpu.VMEM((NC, 2 * NZ, D), BF16),
            pltpu.VMEM((NZ, S, 2 * dhid), BF16),
            pltpu.VMEM((NZ, S, 2 * dhid), BF16),
            pltpu.VMEM((NZ, S, dhid), BF16),
            pltpu.VMEM((NT, R, quarter), BF16),
            pltpu.VMEM((NT, R, quarter), BF16),
            pltpu.VMEM((NZ, S, D // NZ), BF16),
            pltpu.VMEM((NZ, S, D // NZ), BF16),
            pltpu.VMEM((NC, 2 * NZ, quarter), BF16),
            pltpu.VMEM((NC, 2 * NZ, quarter), BF16),
            pltpu.VMEM((NZ, S, quarter), BF16),
            pltpu.VMEM((NZ, S, quarter), BF16),
            dma((len(PHASES), max(NZ, NC, NT))),
            dma((len(PHASES), max(NZ, NC, NT))),
            dma((4,)),
        ],
        compiler_params=pltpu.CompilerParams(collective_id=0, has_side_effects=True, vmem_limit_bytes=60_000_000),
    )(
        tokens, y, zz, group_gain[None], w_out, norm2_gain[None], route_ids, route_weights,
        exp_gate, exp_up, exp_down, dense_gate, dense_up, dense_down.T, branch_gate.reshape(D // 128, 128),
    )
    return mixed, state_next, turned(cx), turned(cb), turned(cc)


def turned(a):
    return jnp.transpose(a, (1, 0, 2))


def solution(mesh):
    NT = mesh.shape["tp"]
    NC = 8 if mesh.shape["ep"] >= 64 else 2
    NZ = mesh.shape["ep"] // NC
    ep = P("ep", None)
    in_specs = (
        ep, P("ep", "tp", None, None), P("ep", None, "tp"), P("ep", None, "tp"), P("ep", None, "tp"),
        P(None, "tp"), P(None, "tp"), P(None, "tp"), P(None, "tp"), P(), P("tp"), P("tp"), P("tp"),
        P(None, "tp"), P(None, "tp"), P(None, "tp"), P(), P("tp"), P("tp", None), P(), ep, ep,
        P("ep", None, "tp"), P("ep", None, "tp"), P("ep", "tp", None), P("ep", "tp"), P("ep", "tp"), P("tp", "ep"), P(),
    )
    out_specs = (P("ep", "tp"), P("ep", "tp", None, None), P("ep", None, "tp"), P("ep", None, "tp"), P("ep", None, "tp"))
    part = functools.partial(body, NZ=NZ, NC=NC, NT=NT, sd=128)
    return jax.shard_map(part, mesh=mesh, in_specs=in_specs, out_specs=out_specs, check_vma=False)
```

```python
import functools

import jax
import jax.numpy as jnp
from jax import lax
from jax.experimental import pallas as pl
from jax.experimental.pallas import tpu as pltpu
from jax.sharding import PartitionSpec as P

EPS = 1e-06
F32 = jnp.float32
BF16 = jnp.bfloat16
HIGH = lax.Precision.HIGHEST
MESH = pl.DeviceIdType.MESH
VMEM_STEP = 24_000_000
VMEM_STORE = 4_000_000


def dot(a, b, **kw):
    return jnp.dot(a, b, preferred_element_type=F32, **kw)


def dot_nt(a, b, **kw):
    return lax.dot_general(a, b, (((1,), (1,)), ((), ())), preferred_element_type=F32, **kw)


def iota(shape, dim):
    return lax.broadcasted_iota(jnp.int32, shape, dim)


def rms_rows(values, gain):
    return values * lax.rsqrt(jnp.mean(values * values, axis=-1, keepdims=True) + EPS) * gain


def silu(v):
    return v * jax.nn.sigmoid(v)


def step_kernel(NE, NC, NT, n_groups, *refs):
    given, refs = refs[:20], refs[20:]
    state, w_x, w_z, w_b, w_c, w_out, w_g, w_u, w_d = refs[:9]
    mixed, state_out, cx_out, cb_out, cc_out = refs[9:14]
    small, refs = refs[14:34], refs[34:]
    tokens, conv_x, conv_b, conv_c, w_dt, dt_bias, a_log, d_skip, taps_x, taps_b, taps_c, gain = small[:12]
    ggain, gain2, ids, wts, dgate, dup, ddown, bgate = small[12:]
    vx, vz, vb, vc, st, vo, vg, vu, vd, pt, dw, dq, tk, cs_, cr, ac, bs_, br, aa, fs_, fr, dout, gs_, gr, lsem, isem, tsem, ssem, rsem = refs
    NZ = NE // NC
    S, D = tokens.shape
    heads, hd, sd = st.shape[1:]
    inner = heads * hd
    per = heads // n_groups
    quarter = D // NT
    planes = NZ // NT
    R = 2 * NE
    e = lax.axis_index("ep")
    t = lax.axis_index("tp")
    z = e // NC
    yc = lax.rem(e, NC)
    q_mine = z // planes
    f_self = q_mine == t

    loads = {}
    for i, (name, src, dst) in enumerate((
        ("x", w_x, vx), ("b", w_b, vb), ("c", w_c, vc), ("z", w_z, vz), ("o", w_out, vo), ("d", w_d.at[0], vd), ("g", w_g.at[0], vg), ("u", w_u.at[0], vu)
    )):
        loads[name] = pltpu.make_async_copy(src, dst, lsem.at[i])
    tiny = [pltpu.make_async_copy(src, dst, tsem.at[i]) for i, (src, dst) in enumerate(zip(given, small))]
    for c in tiny[:12]:
        c.start()
    for name in "xbc":
        loads[name].start()
    ins = [pltpu.make_async_copy(state.at[s], st.at[s], isem.at[s]) for s in range(S)]
    for c in ins:
        c.start()
    for name in "zo":
        loads[name].start()
    for c in tiny[12:]:
        c.start()
    for name in "dgu":
        loads[name].start()

    barrier = pltpu.get_barrier_semaphore()

    def greet(dev):
        pl.semaphore_signal(barrier, inc=1, device_id=dev, device_id_type=MESH)

    def each_ep(count, start):
        def one(k, c):
            half = (k + 1) // 2
            start(lax.rem(e + count // 2 + (1 - 2 * lax.rem(k, 2)) * half, count))
            return c

        lax.fori_loop(0, count - 1, one, 0)

    each_ep(NE, lambda p: greet((p, t)))
    ts = [lax.rem(t + d, NT) for d in range(1, NT)]
    zs = [lax.rem(z + d, NZ) for d in (NZ // 2, *[d for d in range(1, NZ) if d != NZ // 2])]
    cores = [lax.rem(yc + d, NC) for d in range(1, NC)]
    for p in ts:
        greet((e, p))
    for a in range(planes):
        for b in range(NT):
            other_z = t * planes + a

            @pl.when(jnp.logical_or(other_z != z, b != t))
            def _():
                greet((other_z * NC + yc, b))

    PART, DENSE, DOWN, COLS, PRE, ACT, SLOT, HID, DOUT, RET = range(10)

    def send(i, src, dst, dev):
        pltpu.make_async_remote_copy(src_ref=src, dst_ref=dst, send_sem=ssem.at[i], recv_sem=rsem.at[i], device_id=dev, device_id_type=MESH).start()

    def wait(sem, ref, count):
        pltpu.make_async_copy(ref.at[pl.ds(0, count)], ref.at[pl.ds(0, count)], sem).wait()

    def arrive(i, ref, count):
        wait(rsem.at[i], ref, count)

    for c in tiny[:12]:
        c.wait()
    normed = rms_rows(tokens[...].astype(F32), gain[...]).astype(BF16)
    raw = dot_nt(normed, w_dt[...])
    total_heads = raw.shape[1]
    spread_all = (iota((total_heads, inner), 0) == t * heads + iota((total_heads, inner), 1) // hd).astype(F32)
    spread = (iota((heads, inner), 0) == iota((heads, inner), 1) // hd).astype(F32)
    raw = dot(raw, spread_all, precision=HIGH)
    bias = dot(dt_bias[...], spread, precision=HIGH)
    rate = jnp.exp(dot(a_log[...], spread, precision=HIGH))
    skip = dot(d_skip[...], spread, precision=HIGH)
    pre = raw + bias
    step = jnp.maximum(pre, 0.0) + jnp.log1p(jnp.exp(-jnp.abs(pre)))
    decay = jnp.exp(-step * rate)

    def conv(prev, fresh, taps, out):
        fresh = fresh.astype(BF16)
        tap = taps[...].astype(F32)
        depth = prev.shape[0]
        total = fresh.astype(F32) * tap[depth : depth + 1]
        for j in range(depth):
            total = total + prev[j].astype(F32) * tap[j : j + 1]
            out[j] = prev[j + 1] if j + 1 < depth else fresh
        return silu(total)

    loads["x"].wait()
    xs = conv(conv_x, dot(normed, vx[...]), taps_x, cx_out)
    loads["b"].wait()
    bs = conv(conv_b, dot(normed, vb[...]), taps_b, cb_out)
    loads["c"].wait()
    cs = conv(conv_c, dot(normed, vc[...]), taps_c, cc_out)
    inflow = step * xs
    rows = per * hd
    lane = iota((rows, S), 1)
    reads = [jnp.zeros((rows, S), F32) for _ in range(n_groups)]
    for s in range(S):
        ins[s].wait()
        for g in range(n_groups):
            old = st[s, g * per : (g + 1) * per].reshape(rows, sd)
            got = jnp.sum(old * cs[s : s + 1, g * sd : (g + 1) * sd], axis=1, keepdims=True)
            reads[g] = jnp.where(lane == s, got, reads[g])
    loads["z"].wait()
    zz = dot(normed, vz[...]).astype(BF16).astype(F32)
    both = [jnp.sum(bs[:, g * sd : (g + 1) * sd] * cs[:, g * sd : (g + 1) * sd], axis=1, keepdims=True) for g in range(n_groups)]
    for c in tiny[12:]:
        c.wait()
    parts = []
    for g in range(n_groups):
        cut = slice(g * rows, (g + 1) * rows)
        v = decay[:, cut] * reads[g].T + inflow[:, cut] * both[g] + skip[:, cut] * xs[:, cut]
        v = v * silu(zz[:, cut])
        parts.append(v * lax.rsqrt(jnp.mean(v * v, axis=-1, keepdims=True) + EPS) * ggain[:, cut])
    mixed_heads = jnp.concatenate(parts, axis=1).astype(BF16)
    loads["o"].wait()
    pt[t] = dot(mixed_heads, vo[...]).astype(BF16)

    pl.semaphore_wait(barrier, (NE - 1) + (NT - 1) + NZ - f_self.astype(jnp.int32))
    for p in ts:
        send(PART, pt.at[t], pt.at[t], (e, p))
    dw[yc] = jnp.concatenate([dgate[...].astype(F32), dup[...].astype(F32), ddown[...].astype(F32)], axis=1).astype(BF16)
    for p in cores:
        send(DENSE, dw.at[yc], dw.at[yc], (z * NC + p, t))
    loads["d"].wait()
    for p in ts:
        send(DOWN, vd.at[:, pl.ds(pl.multiple_of(p * quarter, quarter), quarter)], dq.at[t], (e, p))
    dq[t] = vd[:, pl.ds(pl.multiple_of(t * quarter, quarter), quarter)]

    slot = iota((S, R), 1)
    named = jnp.zeros((S, R), F32)
    weight = jnp.zeros((S, R), F32)
    for k in range(ids.shape[1]):
        hit = ids[:, k : k + 1] == slot // 2
        named = jnp.where(hit, 1.0, named)
        weight = jnp.where(hit, wts[:, k : k + 1], weight)
    before = (iota((S, S), 0) > iota((S, S), 1)).astype(F32)
    rank = dot(before, named)
    mine = jnp.logical_and(named > 0.5, jnp.abs(rank - lax.rem(slot, 2).astype(F32)) < 0.5)
    take = jnp.where(mine, 1.0, 0.0).T.astype(BF16)
    give = jnp.where(mine, weight, 0.0)

    arrive(PART, pt, NT - 1)
    total = pt[0].astype(F32)
    for k in range(1, NT):
        total = total + pt[k].astype(F32)
    residual = (tokens[...].astype(F32) + total).astype(BF16).astype(F32)
    normed2 = rms_rows(residual, gain2[...]).astype(BF16)
    bs_[...] = dot(take, normed2).astype(BF16).reshape(bs_.shape)
    each_ep(NE, lambda p: send(SLOT, bs_.at[p], br.at[e], (p, t)))
    br[e] = bs_[e]
    depth = D // NZ
    for k in range(NZ):
        fr[k] = normed2[:, k * depth : (k + 1) * depth]
    for p in zs:
        send(COLS, fr.at[p], tk.at[z], (p * NC + yc, t))
    tk[z] = fr[z]

    in_col = inflow.T
    decay_col = decay.T
    for s in range(S):
        for g in range(n_groups):
            cut = slice(g * rows, (g + 1) * rows)
            old = st[s, g * per : (g + 1) * per].reshape(rows, sd)
            new = decay_col[cut, s : s + 1] * old + in_col[cut, s : s + 1] * bs[s : s + 1, g * sd : (g + 1) * sd]
            state_out[s, g * per : (g + 1) * per] = new.reshape(per, hd, sd)

    lanes = bgate.shape[1]
    weighted = jnp.zeros((S, lanes), F32)
    for k in range(bgate.shape[0]):
        weighted = weighted + normed2[:, k * lanes : (k + 1) * lanes].astype(F32) * bgate[k : k + 1, :].astype(F32)
    branch = jax.nn.sigmoid(jnp.sum(weighted, axis=1, keepdims=True))
    own = jnp.zeros((S, quarter), F32)
    for k in range(NT):
        own = jnp.where(t == k, residual[:, k * quarter : (k + 1) * quarter], own)

    def stacked(ref, count):
        return jnp.concatenate([ref[k].astype(F32) for k in range(count)], axis=0).astype(BF16)

    arrive(DENSE, dw, NC - 1)
    arrive(COLS, tk, NZ - 1)
    hid = dw.shape[2] // 3
    plane_w = jnp.concatenate([dw[k] for k in range(NC)], axis=0)
    cs_[...] = dot(stacked(tk, NZ), plane_w[:, : 2 * hid]).reshape(cs_.shape).astype(BF16)
    for p in zs:
        send(PRE, cs_.at[p], cr.at[z], (p * NC + yc, t))
    cr[z] = cs_[z]
    arrive(PRE, cr, NZ - 1)
    pre = cr[0].astype(F32)
    for k in range(1, NZ):
        pre = pre + cr[k].astype(F32)
    ac[z] = (silu(pre[:, :hid]) * pre[:, hid:]).astype(BF16)
    for p in zs:
        send(ACT, ac.at[z], ac.at[z], (p * NC + yc, t))

    loads["g"].wait()
    loads["u"].wait()
    arrive(SLOT, br, NE - 1)
    arrived = br[...].reshape(R, D)
    aa[t] = (silu(dot(arrived, vg[...])) * dot(arrived, vu[...])).astype(BF16)
    for p in ts:
        send(HID, aa.at[t], aa.at[t], (e, p))

    arrive(ACT, ac, NZ - 1)
    wait(ssem.at[COLS], fr, NZ - 1)
    fs_[...] = dot_nt(stacked(ac, NZ), plane_w[:, 2 * hid :]).reshape(fs_.shape).astype(BF16)
    f_slot = lax.rem(z, planes) * NT + t

    def give_dense(k, c):
        @pl.when(jnp.logical_or(z != k, q_mine != t))
        def _():
            send(DOUT, fs_.at[k], dout.at[f_slot], (k * NC + yc, q_mine))

        return c

    lax.fori_loop(0, NZ, give_dense, 0)

    @pl.when(f_self)
    def _():
        dout[f_slot] = fs_[z]

    arrive(DOWN, dq, NT - 1)
    arrive(HID, aa, NT - 1)
    hidden = jnp.concatenate([aa[k] for k in range(NT)], axis=1)
    down = jnp.concatenate([dq[k] for k in range(NT)], axis=0)
    gs_[...] = dot(hidden, down).astype(BF16).reshape(gs_.shape)
    each_ep(NE, lambda p: send(RET, gs_.at[p], gr.at[e], (p, t)))
    gr[e] = gs_[e]

    @pl.when(f_self)
    def _():
        arrive(DOUT, dout, NZ - 1)

    @pl.when(jnp.logical_not(f_self))
    def _():
        arrive(DOUT, dout, NZ)

    dense = []
    for a in range(planes):
        v = dout[a * NT].astype(F32)
        for b in range(1, NT):
            v = v + dout[a * NT + b].astype(F32)
        dense.append(v)
    base = own + branch * jnp.concatenate(dense, axis=1)
    arrive(RET, gr, NE - 1)
    mixed[...] = (base + dot(give.astype(BF16), gr[...].reshape(R, quarter))).astype(BF16)

    for i, ref, count in ((PART, pt, NT - 1), (DENSE, dw, NC - 1), (DOWN, dq, NT - 1), (PRE, cs_, NZ - 1), (ACT, ac, NZ - 1), (SLOT, bs_, NE - 1), (HID, aa, NT - 1), (RET, gs_, NE - 1)):
        wait(ssem.at[i], ref, count)

    @pl.when(f_self)
    def _():
        wait(ssem.at[DOUT], fs_, NZ - 1)

    @pl.when(jnp.logical_not(f_self))
    def _():
        wait(ssem.at[DOUT], fs_, NZ)


def store_kernel(count, *refs):
    ins, outs, sem = refs[:count], refs[count : 2 * count], refs[2 * count]
    copies = [pltpu.make_async_copy(a, b, sem.at[i]) for i, (a, b) in enumerate(zip(ins, outs))]
    for c in copies:
        c.start()
    for c in copies:
        c.wait()


def body(
    tokens, ssm_state, conv_x, conv_b, conv_c, w_x, w_z, w_b, w_c, w_dt, dt_bias, a_log, d_skip, taps_x, taps_b, taps_c,
    norm1_gain, group_gain, w_out, norm2_gain, route_ids, route_weights, exp_gate, exp_up, exp_down, dense_gate, dense_up, dense_down, branch_gate,
    *, NE, NC, NT, sd,
):
    S, D = tokens.shape
    NZ = NE // NC
    inner = w_x.shape[1]
    cols = w_b.shape[1]
    quarter = D // NT
    hidden, dhid = exp_gate.shape[2], dense_gate.shape[1]
    R = 2 * NE
    depth = D // NZ
    vm, hbm, free = (pl.BlockSpec(memory_space=m) for m in (pltpu.VMEM, pltpu.HBM, pl.ANY))
    dma = pltpu.SemaphoreType.DMA
    half = lambda *shape: pltpu.VMEM(shape, BF16)
    shape = jax.ShapeDtypeStruct
    small = (
        tokens, turned(conv_x), turned(conv_b), turned(conv_c), w_dt.T, dt_bias[None], a_log[None], d_skip[None], taps_x, taps_b, taps_c, norm1_gain[None],
        group_gain[None], norm2_gain[None], route_ids, route_weights, dense_gate, dense_up, dense_down.T, branch_gate.reshape(D // 128, 128),
    )
    made = pl.pallas_call(
        functools.partial(step_kernel, NE, NC, NT, cols // sd),
        name="step",
        out_shape=(
            shape((S, quarter), BF16), shape(ssm_state.shape, F32), shape((3, S, inner), BF16), shape((3, S, cols), BF16), shape((3, S, cols), BF16),
        ),
        in_specs=[hbm] * 29,
        out_specs=(vm,) * 5,
        scratch_shapes=[pltpu.VMEM(a.shape, a.dtype) for a in small]
        + [
            half(D, inner), half(D, inner), half(D, cols), half(D, cols), pltpu.VMEM(ssm_state.shape, F32),
            half(inner, D), half(D, hidden), half(D, hidden), half(hidden, D),
            half(NT, S, D), half(NC, dense_gate.shape[0], 3 * dhid), half(NT, hidden, quarter),
            half(NZ, S, depth), half(NZ, S, 2 * dhid), half(NZ, S, 2 * dhid), half(NZ, S, dhid),
            half(NE, 2, D), half(NE, 2, D), half(NT, R, hidden),
            half(NZ, S, depth), half(NZ, S, depth), half(NZ, S, depth),
            half(NE, 2, quarter), half(NE, 2, quarter),
            dma((8,)), dma((S,)), dma((20,)), dma((10,)), dma((10,)),
        ],
        compiler_params=pltpu.CompilerParams(collective_id=0, has_side_effects=True, vmem_limit_bytes=VMEM_STEP),
    )(
        *(fixed(a) for a in small),
        *(fixed(a) for a in (ssm_state, w_x, w_z, w_b, w_c, w_out, exp_gate, exp_up, exp_down)),
    )
    mixed, state_next, cx, cb, cc = pl.pallas_call(
        functools.partial(store_kernel, len(made)),
        name="store",
        out_shape=tuple(shape(a.shape, a.dtype) for a in made),
        in_specs=[free] * len(made),
        out_specs=(hbm,) * len(made),
        scratch_shapes=[dma((len(made),))],
        compiler_params=pltpu.CompilerParams(vmem_limit_bytes=VMEM_STORE),
    )(*made)
    return mixed, state_next, turned(cx), turned(cb), turned(cc)


def fixed(a):
    return pltpu.with_memory_space_constraint(a, pltpu.HBM)


def turned(a):
    return jnp.transpose(a, (1, 0, 2))


def solution(mesh):
    NT = mesh.shape["tp"]
    NC = 8 if mesh.shape["ep"] >= 64 else 2
    NE = mesh.shape["ep"]
    ep = P("ep", None)
    in_specs = (
        ep, P("ep", "tp", None, None), P("ep", None, "tp"), P("ep", None, "tp"), P("ep", None, "tp"),
        P(None, "tp"), P(None, "tp"), P(None, "tp"), P(None, "tp"), P(), P("tp"), P("tp"), P("tp"),
        P(None, "tp"), P(None, "tp"), P(None, "tp"), P(), P("tp"), P("tp", None), P(), ep, ep,
        P("ep", None, "tp"), P("ep", None, "tp"), P("ep", "tp", None), P("ep", "tp"), P("ep", "tp"), P("tp", "ep"), P(),
    )
    out_specs = (P("ep", "tp"), P("ep", "tp", None, None), P("ep", None, "tp"), P("ep", None, "tp"), P("ep", None, "tp"))
    part = functools.partial(body, NE=NE, NC=NC, NT=NT, sd=128)
    return jax.shard_map(part, mesh=mesh, in_specs=in_specs, out_specs=out_specs, check_vma=False)
```

```python
import functools

import jax
import jax.numpy as jnp
from jax import lax
from jax.experimental import pallas as pl
from jax.experimental.pallas import tpu as pltpu
from jax.sharding import PartitionSpec as P

EPS = 1e-06
F32 = jnp.float32
BF16 = jnp.bfloat16
HIGH = lax.Precision.HIGHEST
MESH = pl.DeviceIdType.MESH
VMEM_STEP = 24_000_000
VMEM_STORE = 4_000_000


def dot(a, b, **kw):
    return jnp.dot(a, b, preferred_element_type=F32, **kw)


def dot_nt(a, b, **kw):
    return lax.dot_general(a, b, (((1,), (1,)), ((), ())), preferred_element_type=F32, **kw)


def iota(shape, dim):
    return lax.broadcasted_iota(jnp.int32, shape, dim)


def rms_rows(values, gain):
    return values * lax.rsqrt(jnp.mean(values * values, axis=-1, keepdims=True) + EPS) * gain


def silu(v):
    return v * jax.nn.sigmoid(v)


def step_kernel(NE, NC, NT, n_groups, *refs):
    given, refs = refs[:20], refs[20:]
    state, w_x, w_z, w_b, w_c, w_out, w_g, w_u, w_d = refs[:9]
    mixed, state_out, cx_out, cb_out, cc_out = refs[9:14]
    small, refs = refs[14:34], refs[34:]
    tokens, conv_x, conv_b, conv_c, w_dt, dt_bias, a_log, d_skip, taps_x, taps_b, taps_c, gain = small[:12]
    ggain, gain2, ids, wts, dgate, dup, ddown, bgate = small[12:]
    vx, vz, vb, vc, st, vo, vg, vu, vd, pt, d1, d2, d3, dq, tk, rt, bs_, br, aa, fs_, fr, gs_, gr, lsem, isem, tsem, ssem, rsem = refs
    NZ = NE // NC
    S, D = tokens.shape
    heads, hd, sd = st.shape[1:]
    inner = heads * hd
    per = heads // n_groups
    quarter = D // NT
    R = 2 * NE
    e = lax.axis_index("ep")
    t = lax.axis_index("tp")
    z = e // NC
    yc = lax.rem(e, NC)

    loads = {}
    for i, (name, src, dst) in enumerate((
        ("x", w_x, vx), ("b", w_b, vb), ("c", w_c, vc), ("z", w_z, vz), ("o", w_out, vo), ("d", w_d.at[0], vd), ("g", w_g.at[0], vg), ("u", w_u.at[0], vu)
    )):
        loads[name] = pltpu.make_async_copy(src, dst, lsem.at[i])
    tiny = [pltpu.make_async_copy(src, dst, tsem.at[i]) for i, (src, dst) in enumerate(zip(given, small))]
    for c in tiny[:12]:
        c.start()
    for name in "xbc":
        loads[name].start()
    ins = [pltpu.make_async_copy(state.at[s], st.at[s], isem.at[s]) for s in range(S)]
    for c in ins:
        c.start()
    for name in "zo":
        loads[name].start()
    for c in tiny[12:]:
        c.start()
    for name in "dgu":
        loads[name].start()

    barrier = pltpu.get_barrier_semaphore()

    def greet(dev):
        pl.semaphore_signal(barrier, inc=1, device_id=dev, device_id_type=MESH)

    def each_ep(count, start):
        def one(k, c):
            half = (k + 1) // 2
            start(lax.rem(e + count // 2 + (1 - 2 * lax.rem(k, 2)) * half, count))
            return c

        lax.fori_loop(0, count - 1, one, 0)

    each_ep(NE, lambda p: greet((p, t)))
    ts = [lax.rem(t + d, NT) for d in range(1, NT)]
    zs = [lax.rem(z + d, NZ) for d in (NZ // 2, *[d for d in range(1, NZ) if d != NZ // 2])]
    cores = [lax.rem(yc + d, NC) for d in range(1, NC)]
    for d in range(NZ):
        for p in ts:
            greet((lax.rem(z + d, NZ) * NC + yc, p))

    PART, ROUTE, DENSE, DENSE2, DOWN, TOK, SLOT, DOUT, HID, RET = range(10)

    def send(i, src, dst, dev):
        pltpu.make_async_remote_copy(src_ref=src, dst_ref=dst, send_sem=ssem.at[i], recv_sem=rsem.at[i], device_id=dev, device_id_type=MESH).start()

    def wait(sem, ref, count):
        pltpu.make_async_copy(ref.at[pl.ds(0, count)], ref.at[pl.ds(0, count)], sem).wait()

    def arrive(i, ref, count):
        wait(rsem.at[i], ref, count)

    for c in tiny[:12]:
        c.wait()
    normed = rms_rows(tokens[...].astype(F32), gain[...]).astype(BF16)
    raw = dot_nt(normed, w_dt[...])
    total_heads = raw.shape[1]
    spread_all = (iota((total_heads, inner), 0) == t * heads + iota((total_heads, inner), 1) // hd).astype(F32)
    spread = (iota((heads, inner), 0) == iota((heads, inner), 1) // hd).astype(F32)
    raw = dot(raw, spread_all, precision=HIGH)
    bias = dot(dt_bias[...], spread, precision=HIGH)
    rate = jnp.exp(dot(a_log[...], spread, precision=HIGH))
    skip = dot(d_skip[...], spread, precision=HIGH)
    pre = raw + bias
    step = jnp.maximum(pre, 0.0) + jnp.log1p(jnp.exp(-jnp.abs(pre)))
    decay = jnp.exp(-step * rate)

    def conv(prev, fresh, taps, out):
        fresh = fresh.astype(BF16)
        tap = taps[...].astype(F32)
        depth = prev.shape[0]
        total = fresh.astype(F32) * tap[depth : depth + 1]
        for j in range(depth):
            total = total + prev[j].astype(F32) * tap[j : j + 1]
            out[j] = prev[j + 1] if j + 1 < depth else fresh
        return silu(total)

    loads["x"].wait()
    xs = conv(conv_x, dot(normed, vx[...]), taps_x, cx_out)
    loads["b"].wait()
    bs = conv(conv_b, dot(normed, vb[...]), taps_b, cb_out)
    loads["c"].wait()
    cs = conv(conv_c, dot(normed, vc[...]), taps_c, cc_out)
    inflow = step * xs
    rows = per * hd
    lane = iota((rows, S), 1)
    reads = [jnp.zeros((rows, S), F32) for _ in range(n_groups)]
    for s in range(S):
        ins[s].wait()
        for g in range(n_groups):
            old = st[s, g * per : (g + 1) * per].reshape(rows, sd)
            got = jnp.sum(old * cs[s : s + 1, g * sd : (g + 1) * sd], axis=1, keepdims=True)
            reads[g] = jnp.where(lane == s, got, reads[g])
    loads["z"].wait()
    zz = dot(normed, vz[...]).astype(BF16).astype(F32)
    both = [jnp.sum(bs[:, g * sd : (g + 1) * sd] * cs[:, g * sd : (g + 1) * sd], axis=1, keepdims=True) for g in range(n_groups)]
    for c in tiny[12:]:
        c.wait()
    parts = []
    for g in range(n_groups):
        cut = slice(g * rows, (g + 1) * rows)
        v = decay[:, cut] * reads[g].T + inflow[:, cut] * both[g] + skip[:, cut] * xs[:, cut]
        v = v * silu(zz[:, cut])
        parts.append(v * lax.rsqrt(jnp.mean(v * v, axis=-1, keepdims=True) + EPS) * ggain[:, cut])
    mixed_heads = jnp.concatenate(parts, axis=1).astype(BF16)
    loads["o"].wait()
    pt[t] = dot(mixed_heads, vo[...]).astype(BF16)

    pl.semaphore_wait(barrier, (NE - 1) + NZ * (NT - 1))
    for p in ts:
        send(PART, pt.at[t], pt.at[t], (e, p))

    slot = iota((S, R), 1)
    named = jnp.zeros((S, R), F32)
    weight = jnp.zeros((S, R), F32)
    for k in range(ids.shape[1]):
        hit = ids[:, k : k + 1] == slot // 2
        named = jnp.where(hit, 1.0, named)
        weight = jnp.where(hit, wts[:, k : k + 1], weight)
    before = (iota((S, S), 0) > iota((S, S), 1)).astype(F32)
    rank = dot(before, named)
    mine = jnp.logical_and(named > 0.5, jnp.abs(rank - lax.rem(slot, 2).astype(F32)) < 0.5)
    rt[z] = jnp.where(mine, 1.0, 0.0).astype(BF16)
    give = jnp.where(mine, weight, 0.0)
    hs = dgate.shape[1] // NZ
    lane = iota((dgate.shape[0], 128), 1)
    three = [dgate[...].astype(F32), dup[...].astype(F32), ddown[...].astype(F32)]
    for k in range(NZ):
        page, off = k * hs // 128 * 128, k * hs % 128
        block = jnp.zeros(lane.shape, F32)
        for j, v in enumerate(three):
            v = v[:, page : page + 128]
            shift = (j * hs - off) % 128
            block = jnp.where(jnp.logical_and(lane >= j * hs, lane < (j + 1) * hs), pltpu.roll(v, shift, 1) if shift else v, block)
        d1[k] = block.astype(BF16)
    for p in zs:
        send(ROUTE, rt.at[z], rt.at[z], (p * NC + yc, t))
        send(DENSE, d1.at[p], d2.at[z], (p * NC + yc, t))
    d2[z] = d1[z]
    loads["d"].wait()
    for p in ts:
        send(DOWN, vd.at[:, pl.ds(pl.multiple_of(p * quarter, quarter), quarter)], dq.at[t], (e, p))
    dq[t] = vd[:, pl.ds(pl.multiple_of(t * quarter, quarter), quarter)]

    in_col = inflow.T
    decay_col = decay.T
    for s in range(S):
        for g in range(n_groups):
            cut = slice(g * rows, (g + 1) * rows)
            old = st[s, g * per : (g + 1) * per].reshape(rows, sd)
            new = decay_col[cut, s : s + 1] * old + in_col[cut, s : s + 1] * bs[s : s + 1, g * sd : (g + 1) * sd]
            state_out[s, g * per : (g + 1) * per] = new.reshape(per, hd, sd)

    arrive(PART, pt, NT - 1)
    total = pt[0].astype(F32)
    for k in range(1, NT):
        total = total + pt[k].astype(F32)
    residual = (tokens[...].astype(F32) + total).astype(BF16).astype(F32)
    normed2 = rms_rows(residual, gain2[...]).astype(BF16)
    tk[z] = normed2
    for p in zs:
        send(TOK, tk.at[z], tk.at[z], (p * NC + yc, t))

    arrive(DENSE, d2, NZ - 1)
    for p in cores:
        send(DENSE2, d2, d3.at[:, yc], (z * NC + p, t))
    for k in range(NZ):
        d3[k, yc] = d2[k]

    lanes = bgate.shape[1]
    weighted = jnp.zeros((S, lanes), F32)
    for k in range(bgate.shape[0]):
        weighted = weighted + normed2[:, k * lanes : (k + 1) * lanes].astype(F32) * bgate[k : k + 1, :].astype(F32)
    branch = jax.nn.sigmoid(jnp.sum(weighted, axis=1, keepdims=True))
    own = jnp.zeros((S, quarter), F32)
    for k in range(NT):
        own = jnp.where(t == k, residual[:, k * quarter : (k + 1) * quarter], own)

    def stacked(ref, count):
        return jnp.concatenate([ref[k].astype(F32) for k in range(count)], axis=0).astype(BF16)

    arrive(ROUTE, rt, NZ - 1)
    row, col = iota((R, R), 0), iota((R, R), 1)
    pick = (col == z * 2 * NC + 2 * (row // (2 * NZ)) + lax.rem(row, 2)).astype(BF16)
    same = lax.rem(iota((R, NZ * S), 0) // 2, NZ) == iota((R, NZ * S), 1) // S
    take = jnp.where(same, dot_nt(pick, stacked(rt, NZ)), 0.0).astype(BF16)

    arrive(TOK, tk, NZ - 1)
    toks = stacked(tk, NZ)
    bs_[...] = dot(take, toks).astype(BF16).reshape(bs_.shape)
    for p in cores:
        send(SLOT, bs_.at[p], br.at[yc], (z * NC + p, t))
    br[yc] = bs_[yc]

    arrive(DENSE2, d3, NZ * (NC - 1) // NC)
    dense_w = d3[...].reshape(D, 128)
    pre = dot(toks, dense_w)
    act = silu(pltpu.roll(pre, 2 * hs, 1)) * pltpu.roll(pre, hs, 1)
    lane = iota(act.shape, 1)
    act = jnp.where(jnp.logical_and(lane >= 2 * hs, lane < 3 * hs), act, 0.0).astype(BF16)
    out = dot_nt(act, dense_w)
    for k in range(NZ):
        for j in range(NT):
            fs_[k * NT + j] = out[k * S : (k + 1) * S, j * quarter : (j + 1) * quarter].astype(BF16)
    for d in range(1, NZ * NT):
        p, q = lax.rem(z + d // NT, NZ), lax.rem(t + d % NT, NT)
        send(DOUT, fs_.at[p * NT + q], fr.at[z * NT + t], (p * NC + yc, q))
    fr[z * NT + t] = fs_[z * NT + t]

    loads["g"].wait()
    loads["u"].wait()
    arrive(SLOT, br, NC - 1)
    arrived = br[...].reshape(R, D)
    aa[t] = (silu(dot(arrived, vg[...])) * dot(arrived, vu[...])).astype(BF16)
    for p in ts:
        send(HID, aa.at[t], aa.at[t], (e, p))

    arrive(DOWN, dq, NT - 1)
    down = jnp.concatenate([dq[k] for k in range(NT)], axis=0)
    arrive(HID, aa, NT - 1)
    hidden = jnp.concatenate([aa[k] for k in range(NT)], axis=1)
    gs_[...] = dot(hidden, down).astype(BF16).reshape(gs_.shape)
    each_ep(NE, lambda p: send(RET, gs_.at[lax.rem(p, NC) * NZ + p // NC], gr.at[e], (p, t)))
    gr[e] = gs_[yc * NZ + z]

    arrive(DOUT, fr, NZ * NT - 1)
    dense = jnp.zeros((S, quarter), F32)
    for k in range(NZ * NT):
        dense = dense + fr[k].astype(F32)
    base = own + branch * dense
    arrive(RET, gr, NE - 1)
    mixed[...] = (base + dot(give.astype(BF16), gr[...].reshape(R, quarter))).astype(BF16)

    for i, ref, count in ((PART, pt, NT - 1), (ROUTE, rt, NZ - 1), (DENSE, d1, NZ - 1), (DENSE2, d3, NZ * (NC - 1) // NC), (DOWN, dq, NT - 1), (TOK, tk, NZ - 1), (SLOT, bs_, NC - 1), (HID, aa, NT - 1), (RET, gs_, NE - 1)):
        wait(ssem.at[i], ref, count)
    wait(ssem.at[DOUT], fr, NZ * NT - 1)


def store_kernel(count, *refs):
    ins, outs, sem = refs[:count], refs[count : 2 * count], refs[2 * count]
    copies = [pltpu.make_async_copy(a, b, sem.at[i]) for i, (a, b) in enumerate(zip(ins, outs))]
    for c in copies:
        c.start()
    for c in copies:
        c.wait()


def body(
    tokens, ssm_state, conv_x, conv_b, conv_c, w_x, w_z, w_b, w_c, w_dt, dt_bias, a_log, d_skip, taps_x, taps_b, taps_c,
    norm1_gain, group_gain, w_out, norm2_gain, route_ids, route_weights, exp_gate, exp_up, exp_down, dense_gate, dense_up, dense_down, branch_gate,
    *, NE, NC, NT, sd,
):
    S, D = tokens.shape
    NZ = NE // NC
    inner = w_x.shape[1]
    cols = w_b.shape[1]
    quarter = D // NT
    hidden = exp_gate.shape[2]
    R = 2 * NE
    rows = dense_gate.shape[0]
    vm, hbm, free = (pl.BlockSpec(memory_space=m) for m in (pltpu.VMEM, pltpu.HBM, pl.ANY))
    dma = pltpu.SemaphoreType.DMA
    half = lambda *shape: pltpu.VMEM(shape, BF16)
    shape = jax.ShapeDtypeStruct
    small = (
        tokens, turned(conv_x), turned(conv_b), turned(conv_c), w_dt.T, dt_bias[None], a_log[None], d_skip[None], taps_x, taps_b, taps_c, norm1_gain[None],
        group_gain[None], norm2_gain[None], route_ids, route_weights, dense_gate, dense_up, dense_down.T, branch_gate.reshape(D // 128, 128),
    )
    made = pl.pallas_call(
        functools.partial(step_kernel, NE, NC, NT, cols // sd),
        name="step",
        out_shape=(
            shape((S, quarter), BF16), shape(ssm_state.shape, F32), shape((3, S, inner), BF16), shape((3, S, cols), BF16), shape((3, S, cols), BF16),
        ),
        in_specs=[hbm] * 29,
        out_specs=(vm,) * 5,
        scratch_shapes=[pltpu.VMEM(a.shape, a.dtype) for a in small]
        + [
            half(D, inner), half(D, inner), half(D, cols), half(D, cols), pltpu.VMEM(ssm_state.shape, F32),
            half(inner, D), half(D, hidden), half(D, hidden), half(hidden, D),
            half(NT, S, D), half(NZ, rows, 128), half(NZ, rows, 128), half(NZ, NC, rows, 128), half(NT, hidden, quarter),
            half(NZ, S, D), half(NZ, S, R), half(NC, 2 * NZ, D), half(NC, 2 * NZ, D), half(NT, R, hidden),
            half(NZ * NT, S, quarter), half(NZ * NT, S, quarter),
            half(NE, 2, quarter), half(NE, 2, quarter),
            dma((8,)), dma((S,)), dma((20,)), dma((10,)), dma((10,)),
        ],
        compiler_params=pltpu.CompilerParams(collective_id=0, has_side_effects=True, vmem_limit_bytes=VMEM_STEP),
    )(
        *(fixed(a) for a in small),
        *(fixed(a) for a in (ssm_state, w_x, w_z, w_b, w_c, w_out, exp_gate, exp_up, exp_down)),
    )
    mixed, state_next, cx, cb, cc = pl.pallas_call(
        functools.partial(store_kernel, len(made)),
        name="store",
        out_shape=tuple(shape(a.shape, a.dtype) for a in made),
        in_specs=[free] * len(made),
        out_specs=(hbm,) * len(made),
        scratch_shapes=[dma((len(made),))],
        compiler_params=pltpu.CompilerParams(vmem_limit_bytes=VMEM_STORE),
    )(*made)
    return mixed, state_next, turned(cx), turned(cb), turned(cc)


def fixed(a):
    return pltpu.with_memory_space_constraint(a, pltpu.HBM)


def turned(a):
    return jnp.transpose(a, (1, 0, 2))


def solution(mesh):
    NT = mesh.shape["tp"]
    NC = 8 if mesh.shape["ep"] >= 64 else 2
    NE = mesh.shape["ep"]
    ep = P("ep", None)
    in_specs = (
        ep, P("ep", "tp", None, None), P("ep", None, "tp"), P("ep", None, "tp"), P("ep", None, "tp"),
        P(None, "tp"), P(None, "tp"), P(None, "tp"), P(None, "tp"), P(), P("tp"), P("tp"), P("tp"),
        P(None, "tp"), P(None, "tp"), P(None, "tp"), P(), P("tp"), P("tp", None), P(), ep, ep,
        P("ep", None, "tp"), P("ep", None, "tp"), P("ep", "tp", None), P("ep", "tp"), P("ep", "tp"), P("tp", "ep"), P(),
    )
    out_specs = (P("ep", "tp"), P("ep", "tp", None, None), P("ep", None, "tp"), P("ep", None, "tp"), P("ep", None, "tp"))
    part = functools.partial(body, NE=NE, NC=NC, NT=NT, sd=128)
    return jax.shard_map(part, mesh=mesh, in_specs=in_specs, out_specs=out_specs, check_vma=False)
```

```python
import functools

import jax
import jax.numpy as jnp
from jax import lax
from jax.experimental import pallas as pl
from jax.experimental.pallas import tpu as pltpu
from jax.sharding import PartitionSpec as P

EPS = 1e-06
F32 = jnp.float32
BF16 = jnp.bfloat16
HIGH = lax.Precision.HIGHEST
MESH = pl.DeviceIdType.MESH
VMEM_STEP = 24_000_000
VMEM_STORE = 4_000_000


def dot(a, b, **kw):
    return jnp.dot(a, b, preferred_element_type=F32, **kw)


def dot_nt(a, b, **kw):
    return lax.dot_general(a, b, (((1,), (1,)), ((), ())), preferred_element_type=F32, **kw)


def iota(shape, dim):
    return lax.broadcasted_iota(jnp.int32, shape, dim)


def rms_rows(values, gain):
    return values * lax.rsqrt(jnp.mean(values * values, axis=-1, keepdims=True) + EPS) * gain


def silu(v):
    return v * jax.nn.sigmoid(v)


def step_kernel(NE, NC, NT, n_groups, *refs):
    given, refs = refs[:20], refs[20:]
    state, w_x, w_z, w_b, w_c, w_out, w_g, w_u, w_d = refs[:9]
    mixed, state_out, cx_out, cb_out, cc_out = refs[9:14]
    small, refs = refs[14:34], refs[34:]
    tokens, conv_x, conv_b, conv_c, w_dt, dt_bias, a_log, d_skip, taps_x, taps_b, taps_c, gain = small[:12]
    ggain, gain2, ids, wts, dgate, dup, ddown, bgate = small[12:]
    vx, vz, vb, vc, st, vo, vg, vu, vd, pt, d1, d2, d3, dq, tk, rt, bs_, br, aa, fs_, fr, gs_, gr, lsem, isem, tsem, ssem, rsem = refs
    NZ = NE // NC
    S, D = tokens.shape
    heads, hd, sd = st.shape[1:]
    inner = heads * hd
    per = heads // n_groups
    quarter = D // NT
    R = 2 * NE
    e = lax.axis_index("ep")
    t = lax.axis_index("tp")
    z = e // NC
    yc = lax.rem(e, NC)

    loads = {}
    for i, (name, src, dst) in enumerate((
        ("x", w_x, vx), ("b", w_b, vb), ("c", w_c, vc), ("z", w_z, vz), ("o", w_out, vo), ("d", w_d.at[0], vd), ("g", w_g.at[0], vg), ("u", w_u.at[0], vu)
    )):
        loads[name] = pltpu.make_async_copy(src, dst, lsem.at[i])
    tiny = [pltpu.make_async_copy(src, dst, tsem.at[i]) for i, (src, dst) in enumerate(zip(given, small))]
    for c in tiny[:12]:
        c.start()
    for name in "xbc":
        loads[name].start()
    ins = [pltpu.make_async_copy(state.at[s], st.at[s], isem.at[s]) for s in range(S)]
    for c in ins:
        c.start()
    for name in "zo":
        loads[name].start()
    for c in tiny[12:]:
        c.start()
    for name in "dgu":
        loads[name].start()

    barrier = pltpu.get_barrier_semaphore()

    def greet(dev):
        pl.semaphore_signal(barrier, inc=1, device_id=dev, device_id_type=MESH)

    def each_ep(count, start):
        def one(k, c):
            half = (k + 1) // 2
            start(lax.rem(e + count // 2 + (1 - 2 * lax.rem(k, 2)) * half, count))
            return c

        lax.fori_loop(0, count - 1, one, 0)

    each_ep(NE, lambda p: greet((p, t)))
    ts = [lax.rem(t + d, NT) for d in range(1, NT)]
    ring = sorted(range(NZ), key=lambda d: (min(d, NZ - d), d))
    half = NZ // 2
    groups = (ring[:half], ring[half:])
    at = [lax.rem(z + d, NZ) for d in range(NZ)]
    zs = [at[d] for d in reversed(ring) if d]
    cores = [lax.rem(yc + d, NC) for d in range(1, NC)]
    for d in range(NZ):
        for p in ts:
            greet((lax.rem(z + d, NZ) * NC + yc, p))

    PART, ROUTE, DENSE, DENSE2, DOWN, TOK, SLOT, DOUT, HID, RET, TOK2, SLOT2, HID2 = range(13)

    def send(i, src, dst, dev, there=None):
        pltpu.make_async_remote_copy(src_ref=src, dst_ref=dst, send_sem=ssem.at[i], recv_sem=rsem.at[i if there is None else there], device_id=dev, device_id_type=MESH).start()

    def wait(sem, ref, count):
        pltpu.make_async_copy(ref.at[pl.ds(0, count)], ref.at[pl.ds(0, count)], sem).wait()

    def arrive(i, ref, count):
        wait(rsem.at[i], ref, count)

    for c in tiny[:12]:
        c.wait()
    normed = rms_rows(tokens[...].astype(F32), gain[...]).astype(BF16)
    raw = dot_nt(normed, w_dt[...])
    total_heads = raw.shape[1]
    spread_all = (iota((total_heads, inner), 0) == t * heads + iota((total_heads, inner), 1) // hd).astype(F32)
    spread = (iota((heads, inner), 0) == iota((heads, inner), 1) // hd).astype(F32)
    raw = dot(raw, spread_all, precision=HIGH)
    bias = dot(dt_bias[...], spread, precision=HIGH)
    rate = jnp.exp(dot(a_log[...], spread, precision=HIGH))
    skip = dot(d_skip[...], spread, precision=HIGH)
    pre = raw + bias
    step = jnp.maximum(pre, 0.0) + jnp.log1p(jnp.exp(-jnp.abs(pre)))
    decay = jnp.exp(-step * rate)

    def conv(prev, fresh, taps, out):
        fresh = fresh.astype(BF16)
        tap = taps[...].astype(F32)
        depth = prev.shape[0]
        total = fresh.astype(F32) * tap[depth : depth + 1]
        for j in range(depth):
            total = total + prev[j].astype(F32) * tap[j : j + 1]
            out[j] = prev[j + 1] if j + 1 < depth else fresh
        return silu(total)

    loads["x"].wait()
    xs = conv(conv_x, dot(normed, vx[...]), taps_x, cx_out)
    loads["b"].wait()
    bs = conv(conv_b, dot(normed, vb[...]), taps_b, cb_out)
    loads["c"].wait()
    cs = conv(conv_c, dot(normed, vc[...]), taps_c, cc_out)
    inflow = step * xs
    rows = per * hd
    lane = iota((rows, S), 1)
    reads = [jnp.zeros((rows, S), F32) for _ in range(n_groups)]
    for s in range(S):
        ins[s].wait()
        for g in range(n_groups):
            old = st[s, g * per : (g + 1) * per].reshape(rows, sd)
            got = jnp.sum(old * cs[s : s + 1, g * sd : (g + 1) * sd], axis=1, keepdims=True)
            reads[g] = jnp.where(lane == s, got, reads[g])
    loads["z"].wait()
    zz = dot(normed, vz[...]).astype(BF16).astype(F32)
    both = [jnp.sum(bs[:, g * sd : (g + 1) * sd] * cs[:, g * sd : (g + 1) * sd], axis=1, keepdims=True) for g in range(n_groups)]
    for c in tiny[12:]:
        c.wait()
    parts = []
    for g in range(n_groups):
        cut = slice(g * rows, (g + 1) * rows)
        v = decay[:, cut] * reads[g].T + inflow[:, cut] * both[g] + skip[:, cut] * xs[:, cut]
        v = v * silu(zz[:, cut])
        parts.append(v * lax.rsqrt(jnp.mean(v * v, axis=-1, keepdims=True) + EPS) * ggain[:, cut])
    mixed_heads = jnp.concatenate(parts, axis=1).astype(BF16)
    loads["o"].wait()
    pt[t] = dot(mixed_heads, vo[...]).astype(BF16)

    pl.semaphore_wait(barrier, (NE - 1) + NZ * (NT - 1))
    for p in ts:
        send(PART, pt.at[t], pt.at[t], (e, p))

    slot = iota((S, R), 1)
    named = jnp.zeros((S, R), F32)
    weight = jnp.zeros((S, R), F32)
    for k in range(ids.shape[1]):
        hit = ids[:, k : k + 1] == slot // 2
        named = jnp.where(hit, 1.0, named)
        weight = jnp.where(hit, wts[:, k : k + 1], weight)
    before = (iota((S, S), 0) > iota((S, S), 1)).astype(F32)
    rank = dot(before, named)
    mine = jnp.logical_and(named > 0.5, jnp.abs(rank - lax.rem(slot, 2).astype(F32)) < 0.5)
    rt[z] = jnp.where(mine, 1.0, 0.0).astype(BF16)
    give = jnp.where(mine, weight, 0.0)
    hs = dgate.shape[1] // NZ
    lane = iota((dgate.shape[0], 128), 1)
    three = [dgate[...].astype(F32), dup[...].astype(F32), ddown[...].astype(F32)]
    for k in range(NZ):
        page, off = k * hs // 128 * 128, k * hs % 128
        block = jnp.zeros(lane.shape, F32)
        for j, v in enumerate(three):
            v = v[:, page : page + 128]
            shift = (j * hs - off) % 128
            block = jnp.where(jnp.logical_and(lane >= j * hs, lane < (j + 1) * hs), pltpu.roll(v, shift, 1) if shift else v, block)
        d1[k] = block.astype(BF16)
    for p in zs:
        send(ROUTE, rt.at[z], rt.at[z], (p * NC + yc, t))
        send(DENSE, d1.at[p], d2.at[z], (p * NC + yc, t))
    d2[z] = d1[z]
    loads["d"].wait()
    for p in ts:
        send(DOWN, vd.at[:, pl.ds(pl.multiple_of(p * quarter, quarter), quarter)], dq.at[t], (e, p))
    dq[t] = vd[:, pl.ds(pl.multiple_of(t * quarter, quarter), quarter)]

    in_col = inflow.T
    decay_col = decay.T
    for s in range(S):
        for g in range(n_groups):
            cut = slice(g * rows, (g + 1) * rows)
            old = st[s, g * per : (g + 1) * per].reshape(rows, sd)
            new = decay_col[cut, s : s + 1] * old + in_col[cut, s : s + 1] * bs[s : s + 1, g * sd : (g + 1) * sd]
            state_out[s, g * per : (g + 1) * per] = new.reshape(per, hd, sd)

    arrive(PART, pt, NT - 1)
    total = pt[0].astype(F32)
    for k in range(1, NT):
        total = total + pt[k].astype(F32)
    residual = (tokens[...].astype(F32) + total).astype(BF16).astype(F32)
    normed2 = rms_rows(residual, gain2[...]).astype(BF16)
    tk[z] = normed2
    for d in reversed(ring[1:]):
        send(TOK, tk.at[z], tk.at[z], (at[d] * NC + yc, t), TOK2 if (NZ - d) % NZ in groups[1] else TOK)

    arrive(DENSE, d2, NZ - 1)
    for p in cores:
        send(DENSE2, d2, d3.at[:, yc], (z * NC + p, t))
    for k in range(NZ):
        d3[k, yc] = d2[k]

    lanes = bgate.shape[1]
    weighted = jnp.zeros((S, lanes), F32)
    for k in range(bgate.shape[0]):
        weighted = weighted + normed2[:, k * lanes : (k + 1) * lanes].astype(F32) * bgate[k : k + 1, :].astype(F32)
    branch = jax.nn.sigmoid(jnp.sum(weighted, axis=1, keepdims=True))
    own = jnp.zeros((S, quarter), F32)
    for k in range(NT):
        own = jnp.where(t == k, residual[:, k * quarter : (k + 1) * quarter], own)

    def stacked(ref, offsets):
        return jnp.concatenate([ref[at[d]].astype(F32) for d in offsets], axis=0).astype(BF16)

    arrive(ROUTE, rt, NZ - 1)
    rows_g = NC * half * 2
    row, col = iota((rows_g, R), 0), iota((rows_g, R), 1)
    pick = (col == z * 2 * NC + 2 * (row // (2 * half)) + lax.rem(row, 2)).astype(BF16)
    same = lax.rem(iota((rows_g, half * S), 0) // 2, half) == iota((rows_g, half * S), 1) // S
    takes = [jnp.where(same, dot_nt(pick, stacked(rt, group)), 0.0).astype(BF16) for group in groups]

    toks = []
    for k, group in enumerate(groups):
        arrive((TOK, TOK2)[k], tk, len(group) - (k == 0))
        toks.append(stacked(tk, group))
        bs_[k] = dot(takes[k], toks[k]).astype(BF16).reshape(bs_.shape[1:])
        for p in cores:
            send((SLOT, SLOT2)[k], bs_.at[k, p], br.at[k, yc], (z * NC + p, t))
        br[k, yc] = bs_[k, yc]

    arrive(DENSE2, d3, NZ * (NC - 1) // NC)
    dense_w = d3[...].reshape(D, 128)
    pre = dot(jnp.concatenate(toks, axis=0), dense_w)
    act = silu(pltpu.roll(pre, 2 * hs, 1)) * pltpu.roll(pre, hs, 1)
    lane = iota(act.shape, 1)
    act = jnp.where(jnp.logical_and(lane >= 2 * hs, lane < 3 * hs), act, 0.0).astype(BF16)
    out = dot_nt(act, dense_w)
    for k in range(NZ):
        for j in range(NT):
            fs_[k * NT + j] = out[k * S : (k + 1) * S, j * quarter : (j + 1) * quarter].astype(BF16)
    for k in reversed(range(NZ)):
        for d in range(NT):
            if ring[k] or d:
                q = lax.rem(t + d, NT)
                send(DOUT, fs_.at[k * NT + q], fr.at[z * NT + t], (at[ring[k]] * NC + yc, q))
    fr[z * NT + t] = fs_[t]

    loads["g"].wait()
    loads["u"].wait()
    for k in range(2):
        arrive((SLOT, SLOT2)[k], br.at[k], NC - 1)
        arrived = br[k].reshape(rows_g, D)
        aa[k, t] = (silu(dot(arrived, vg[...])) * dot(arrived, vu[...])).astype(BF16)
        for p in ts:
            send((HID, HID2)[k], aa.at[k, t], aa.at[k, t], (e, p))

    arrive(DOWN, dq, NT - 1)
    down = jnp.concatenate([dq[k] for k in range(NT)], axis=0)
    for k, group in enumerate(groups):
        arrive((HID, HID2)[k], aa.at[k], NT - 1)
        hidden = jnp.concatenate([aa[k, j] for j in range(NT)], axis=1)
        gs_[k] = dot(hidden, down).astype(BF16).reshape(gs_.shape[1:])
        for i in reversed(range(half)):

            def back(j, c):
                p = lax.rem(yc + j, NC)
                send(RET, gs_.at[k, p * half + i], gr.at[e], (at[group[i]] * NC + p, t))
                return c

            lax.fori_loop(0 if group[i] else 1, NC, back, 0)
    gr[e] = gs_[0, yc * half]

    arrive(DOUT, fr, NZ * NT - 1)
    dense = jnp.zeros((S, quarter), F32)
    for k in range(NZ * NT):
        dense = dense + fr[k].astype(F32)
    base = own + branch * dense
    arrive(RET, gr, NE - 1)
    mixed[...] = (base + dot(give.astype(BF16), gr[...].reshape(R, quarter))).astype(BF16)

    for i, ref, count in ((PART, pt, NT - 1), (ROUTE, rt, NZ - 1), (DENSE, d1, NZ - 1), (DENSE2, d3, NZ * (NC - 1) // NC), (DOWN, dq, NT - 1), (TOK, tk, NZ - 1), (SLOT, bs_.at[0], NC - 1), (SLOT2, bs_.at[1], NC - 1), (HID, aa.at[0], NT - 1), (HID2, aa.at[1], NT - 1), (RET, gr, NE - 1)):
        wait(ssem.at[i], ref, count)
    wait(ssem.at[DOUT], fr, NZ * NT - 1)


def store_kernel(count, *refs):
    ins, outs, sem = refs[:count], refs[count : 2 * count], refs[2 * count]
    copies = [pltpu.make_async_copy(a, b, sem.at[i]) for i, (a, b) in enumerate(zip(ins, outs))]
    for c in copies:
        c.start()
    for c in copies:
        c.wait()


def body(
    tokens, ssm_state, conv_x, conv_b, conv_c, w_x, w_z, w_b, w_c, w_dt, dt_bias, a_log, d_skip, taps_x, taps_b, taps_c,
    norm1_gain, group_gain, w_out, norm2_gain, route_ids, route_weights, exp_gate, exp_up, exp_down, dense_gate, dense_up, dense_down, branch_gate,
    *, NE, NC, NT, sd,
):
    S, D = tokens.shape
    NZ = NE // NC
    inner = w_x.shape[1]
    cols = w_b.shape[1]
    quarter = D // NT
    hidden = exp_gate.shape[2]
    R = 2 * NE
    rows = dense_gate.shape[0]
    vm, hbm, free = (pl.BlockSpec(memory_space=m) for m in (pltpu.VMEM, pltpu.HBM, pl.ANY))
    dma = pltpu.SemaphoreType.DMA
    half = lambda *shape: pltpu.VMEM(shape, BF16)
    shape = jax.ShapeDtypeStruct
    small = (
        tokens, turned(conv_x), turned(conv_b), turned(conv_c), w_dt.T, dt_bias[None], a_log[None], d_skip[None], taps_x, taps_b, taps_c, norm1_gain[None],
        group_gain[None], norm2_gain[None], route_ids, route_weights, dense_gate, dense_up, dense_down.T, branch_gate.reshape(D // 128, 128),
    )
    made = pl.pallas_call(
        functools.partial(step_kernel, NE, NC, NT, cols // sd),
        name="step",
        out_shape=(
            shape((S, quarter), BF16), shape(ssm_state.shape, F32), shape((3, S, inner), BF16), shape((3, S, cols), BF16), shape((3, S, cols), BF16),
        ),
        in_specs=[hbm] * 29,
        out_specs=(vm,) * 5,
        scratch_shapes=[pltpu.VMEM(a.shape, a.dtype) for a in small]
        + [
            half(D, inner), half(D, inner), half(D, cols), half(D, cols), pltpu.VMEM(ssm_state.shape, F32),
            half(inner, D), half(D, hidden), half(D, hidden), half(hidden, D),
            half(NT, S, D), half(NZ, rows, 128), half(NZ, rows, 128), half(NZ, NC, rows, 128), half(NT, hidden, quarter),
            half(NZ, S, D), half(NZ, S, R), half(2, NC, NZ, D), half(2, NC, NZ, D), half(2, NT, R // 2, hidden),
            half(NZ * NT, S, quarter), half(NZ * NT, S, quarter),
            half(2, NE // 2, 2, quarter), half(NE, 2, quarter),
            dma((8,)), dma((S,)), dma((20,)), dma((13,)), dma((13,)),
        ],
        compiler_params=pltpu.CompilerParams(collective_id=0, has_side_effects=True, vmem_limit_bytes=VMEM_STEP),
    )(
        *(fixed(a) for a in small),
        *(fixed(a) for a in (ssm_state, w_x, w_z, w_b, w_c, w_out, exp_gate, exp_up, exp_down)),
    )
    mixed, state_next, cx, cb, cc = pl.pallas_call(
        functools.partial(store_kernel, len(made)),
        name="store",
        out_shape=tuple(shape(a.shape, a.dtype) for a in made),
        in_specs=[free] * len(made),
        out_specs=(hbm,) * len(made),
        scratch_shapes=[dma((len(made),))],
        compiler_params=pltpu.CompilerParams(vmem_limit_bytes=VMEM_STORE),
    )(*made)
    return mixed, state_next, turned(cx), turned(cb), turned(cc)


def fixed(a):
    return pltpu.with_memory_space_constraint(a, pltpu.HBM)


def turned(a):
    return jnp.transpose(a, (1, 0, 2))


def solution(mesh):
    NT = mesh.shape["tp"]
    NC = 8 if mesh.shape["ep"] >= 64 else 2
    NE = mesh.shape["ep"]
    ep = P("ep", None)
    in_specs = (
        ep, P("ep", "tp", None, None), P("ep", None, "tp"), P("ep", None, "tp"), P("ep", None, "tp"),
        P(None, "tp"), P(None, "tp"), P(None, "tp"), P(None, "tp"), P(), P("tp"), P("tp"), P("tp"),
        P(None, "tp"), P(None, "tp"), P(None, "tp"), P(), P("tp"), P("tp", None), P(), ep, ep,
        P("ep", None, "tp"), P("ep", None, "tp"), P("ep", "tp", None), P("ep", "tp"), P("ep", "tp"), P("tp", "ep"), P(),
    )
    out_specs = (P("ep", "tp"), P("ep", "tp", None, None), P("ep", None, "tp"), P("ep", None, "tp"), P("ep", None, "tp"))
    part = functools.partial(body, NE=NE, NC=NC, NT=NT, sd=128)
    return jax.shard_map(part, mesh=mesh, in_specs=in_specs, out_specs=out_specs, check_vma=False)
```

```python
import functools

import jax
import jax.numpy as jnp
from jax import lax
from jax.experimental import pallas as pl
from jax.experimental.pallas import tpu as pltpu
from jax.sharding import PartitionSpec as P

EPS = 1e-06
F32 = jnp.float32
BF16 = jnp.bfloat16
HIGH = lax.Precision.HIGHEST
MESH = pl.DeviceIdType.MESH
VMEM_STEP = 24_000_000
VMEM_STORE = 4_000_000


def dot(a, b, **kw):
    return jnp.dot(a, b, preferred_element_type=F32, **kw)


def dot_nt(a, b, **kw):
    return lax.dot_general(a, b, (((1,), (1,)), ((), ())), preferred_element_type=F32, **kw)


def iota(shape, dim):
    return lax.broadcasted_iota(jnp.int32, shape, dim)


def rms_rows(values, gain):
    return values * lax.rsqrt(jnp.mean(values * values, axis=-1, keepdims=True) + EPS) * gain


def silu(v):
    return v * jax.nn.sigmoid(v)


def step_kernel(NE, NC, NT, n_groups, *refs):
    given, refs = refs[:20], refs[20:]
    state, w_x, w_z, w_b, w_c, w_out, w_g, w_u, w_d = refs[:9]
    mixed, state_out, cx_out, cb_out, cc_out = refs[9:14]
    small, refs = refs[14:34], refs[34:]
    tokens, conv_x, conv_b, conv_c, w_dt, dt_bias, a_log, d_skip, taps_x, taps_b, taps_c, gain = small[:12]
    ggain, gain2, ids, wts, dgate, dup, ddown, bgate = small[12:]
    vx, vz, vb, vc, st, vo, vg, vu, vd, pt, d1, d2, d3, dq, tk, rt, bs_, br, aa, fs_, fr, gs_, gr, lsem, isem, tsem, ssem, rsem = refs
    NZ = NE // NC
    S, D = tokens.shape
    heads, hd, sd = st.shape[1:]
    inner = heads * hd
    per = heads // n_groups
    quarter = D // NT
    R = 2 * NE
    e = lax.axis_index("ep")
    t = lax.axis_index("tp")
    z = e // NC
    yc = lax.rem(e, NC)

    ts = [lax.rem(t + d, NT) for d in range(1, NT)]
    ring = sorted(range(NZ), key=lambda d: (min(d, NZ - d), d))
    half = NZ // 2
    groups = (ring[:half], ring[half:])
    at = [lax.rem(z + d, NZ) for d in range(NZ)]
    zs = [at[d] for d in reversed(ring) if d]
    around = [lax.rem(yc + d, NC) for d in range(NC)]
    cores = around[1:]
    barrier = pltpu.get_barrier_semaphore()
    for dev in [(p * NC + yc, t) for p in zs] + [(z * NC + p, t) for p in cores] + [(e, p) for p in ts]:
        pl.semaphore_signal(barrier, inc=1, device_id=dev, device_id_type=MESH)

    loads = {}
    for i, (name, src, dst) in enumerate((
        ("x", w_x, vx), ("b", w_b, vb), ("c", w_c, vc), ("z", w_z, vz), ("o", w_out, vo), ("d", w_d.at[0], vd), ("g", w_g.at[0], vg), ("u", w_u.at[0], vu)
    )):
        loads[name] = pltpu.make_async_copy(src, dst, lsem.at[i])
    tiny = [pltpu.make_async_copy(src, dst, tsem.at[i]) for i, (src, dst) in enumerate(zip(given, small))]
    for c in tiny[:12]:
        c.start()
    for name in "xbcz":
        loads[name].start()
    ins = [pltpu.make_async_copy(state.at[s], st.at[s], isem.at[s]) for s in range(S)]
    for c in ins:
        c.start()
    loads["o"].start()
    for c in tiny[12:]:
        c.start()
    for name in "dgu":
        loads[name].start()

    PART, ROUTE, DENSE, DENSE2, DOWN, TOK, SLOT, DOUT, HID, RET, TOK2, SLOT2, HID2 = range(13)

    def send(i, src, dst, dev, there=None):
        pltpu.make_async_remote_copy(src_ref=src, dst_ref=dst, send_sem=ssem.at[i], recv_sem=rsem.at[i if there is None else there], device_id=dev, device_id_type=MESH).start()

    def wait(sem, ref, count):
        pltpu.make_async_copy(ref.at[pl.ds(0, count)], ref.at[pl.ds(0, count)], sem).wait()

    def arrive(i, ref, count):
        wait(rsem.at[i], ref, count)

    for c in tiny[:12]:
        c.wait()
    normed = rms_rows(tokens[...].astype(F32), gain[...]).astype(BF16)
    raw = dot_nt(normed, w_dt[...])
    total_heads = raw.shape[1]
    spread_all = (iota((total_heads, inner), 0) == t * heads + iota((total_heads, inner), 1) // hd).astype(F32)
    spread = (iota((heads, inner), 0) == iota((heads, inner), 1) // hd).astype(F32)
    raw = dot(raw, spread_all, precision=HIGH)
    bias = dot(dt_bias[...], spread, precision=HIGH)
    rate = jnp.exp(dot(a_log[...], spread, precision=HIGH))
    skip = dot(d_skip[...], spread, precision=HIGH)
    pre = raw + bias
    step = jnp.maximum(pre, 0.0) + jnp.log1p(jnp.exp(-jnp.abs(pre)))
    decay = jnp.exp(-step * rate)

    def conv(prev, fresh, taps, out):
        fresh = fresh.astype(BF16)
        tap = taps[...].astype(F32)
        depth = prev.shape[0]
        total = fresh.astype(F32) * tap[depth : depth + 1]
        for j in range(depth):
            total = total + prev[j].astype(F32) * tap[j : j + 1]
            out[j] = prev[j + 1] if j + 1 < depth else fresh
        return silu(total)

    for name in "xbc":
        loads[name].wait()
    xs = conv(conv_x, dot(normed, vx[...]), taps_x, cx_out)
    bs = conv(conv_b, dot(normed, vb[...]), taps_b, cb_out)
    cs = conv(conv_c, dot(normed, vc[...]), taps_c, cc_out)
    inflow = step * xs
    loads["z"].wait()
    zz = dot(normed, vz[...]).astype(BF16).astype(F32)
    rows = per * hd
    lane = iota((rows, S), 1)
    reads = [jnp.zeros((rows, S), F32) for _ in range(n_groups)]
    for s in range(S):
        if s % 4 == 0:
            for c in ins[s : s + 4]:
                c.wait()
        for g in range(n_groups):
            old = st[s, g * per : (g + 1) * per].reshape(rows, sd)
            got = jnp.sum(old * cs[s : s + 1, g * sd : (g + 1) * sd], axis=1, keepdims=True)
            reads[g] = jnp.where(lane == s, got, reads[g])
    both = [jnp.sum(bs[:, g * sd : (g + 1) * sd] * cs[:, g * sd : (g + 1) * sd], axis=1, keepdims=True) for g in range(n_groups)]
    for c in tiny[12:]:
        c.wait()
    parts = []
    for g in range(n_groups):
        cut = slice(g * rows, (g + 1) * rows)
        v = decay[:, cut] * reads[g].T + inflow[:, cut] * both[g] + skip[:, cut] * xs[:, cut]
        v = v * silu(zz[:, cut])
        parts.append(v * lax.rsqrt(jnp.mean(v * v, axis=-1, keepdims=True) + EPS) * ggain[:, cut])
    mixed_heads = jnp.concatenate(parts, axis=1).astype(BF16)
    loads["o"].wait()
    pt[t] = dot(mixed_heads, vo[...]).astype(BF16)

    pl.semaphore_wait(barrier, (NZ - 1) + (NC - 1) + (NT - 1))
    for p in ts:
        send(PART, pt.at[t], pt.at[t], (e, p))

    slot = iota((S, R), 1)
    named = jnp.zeros((S, R), F32)
    weight = jnp.zeros((S, R), F32)
    for k in range(ids.shape[1]):
        hit = ids[:, k : k + 1] == slot // 2
        named = jnp.where(hit, 1.0, named)
        weight = jnp.where(hit, wts[:, k : k + 1], weight)
    before = (iota((S, S), 0) > iota((S, S), 1)).astype(F32)
    rank = dot(before, named)
    mine = jnp.logical_and(named > 0.5, jnp.abs(rank - lax.rem(slot, 2).astype(F32)) < 0.5)
    rt[z] = jnp.where(mine, 1.0, 0.0).astype(BF16)
    give = jnp.where(mine, weight, 0.0)
    hs = dgate.shape[1] // NZ
    lane = iota((dgate.shape[0], 128), 1)
    three = [dgate[...].astype(F32), dup[...].astype(F32), ddown[...].astype(F32)]
    for k in range(NZ):
        page, off = k * hs // 128 * 128, k * hs % 128
        block = jnp.zeros(lane.shape, F32)
        for j, v in enumerate(three):
            v = v[:, page : page + 128]
            shift = (j * hs - off) % 128
            block = jnp.where(jnp.logical_and(lane >= j * hs, lane < (j + 1) * hs), pltpu.roll(v, shift, 1) if shift else v, block)
        d1[k] = block.astype(BF16)
    for p in zs:
        send(ROUTE, rt.at[z], rt.at[z], (p * NC + yc, t))
        send(DENSE, d1.at[p], d2.at[z], (p * NC + yc, t))
    d2[z] = d1[z]
    loads["d"].wait()
    for p in ts:
        send(DOWN, vd.at[:, pl.ds(pl.multiple_of(p * quarter, quarter), quarter)], dq.at[t], (e, p))
    dq[t] = vd[:, pl.ds(pl.multiple_of(t * quarter, quarter), quarter)]

    in_col = inflow.T
    decay_col = decay.T
    for s in range(S):
        for g in range(n_groups):
            cut = slice(g * rows, (g + 1) * rows)
            old = st[s, g * per : (g + 1) * per].reshape(rows, sd)
            new = decay_col[cut, s : s + 1] * old + in_col[cut, s : s + 1] * bs[s : s + 1, g * sd : (g + 1) * sd]
            state_out[s, g * per : (g + 1) * per] = new.reshape(per, hd, sd)

    arrive(PART, pt, NT - 1)
    total = pt[0].astype(F32)
    for k in range(1, NT):
        total = total + pt[k].astype(F32)
    residual = (tokens[...].astype(F32) + total).astype(BF16).astype(F32)
    normed2 = rms_rows(residual, gain2[...]).astype(BF16)
    tk[z] = normed2
    for d in reversed(ring[1:]):
        send(TOK, tk.at[z], tk.at[z], (at[d] * NC + yc, t), TOK2 if (NZ - d) % NZ in groups[1] else TOK)

    arrive(DENSE, d2, NZ - 1)
    for p in cores:
        send(DENSE2, d2, d3.at[:, yc], (z * NC + p, t))
    for k in range(NZ):
        d3[k, yc] = d2[k]

    lanes = bgate.shape[1]
    weighted = jnp.zeros((S, lanes), F32)
    for k in range(bgate.shape[0]):
        weighted = weighted + normed2[:, k * lanes : (k + 1) * lanes].astype(F32) * bgate[k : k + 1, :].astype(F32)
    branch = jax.nn.sigmoid(jnp.sum(weighted, axis=1, keepdims=True))
    own = jnp.zeros((S, quarter), F32)
    for k in range(NT):
        own = jnp.where(t == k, residual[:, k * quarter : (k + 1) * quarter], own)

    def stacked(ref, offsets):
        return jnp.concatenate([ref[at[d]].astype(F32) for d in offsets], axis=0).astype(BF16)

    arrive(ROUTE, rt, NZ - 1)
    rows_g = NC * half * 2
    row, col = iota((rows_g, R), 0), iota((rows_g, R), 1)
    pick = (col == z * 2 * NC + 2 * (row // (2 * half)) + lax.rem(row, 2)).astype(BF16)
    same = lax.rem(iota((rows_g, half * S), 0) // 2, half) == iota((rows_g, half * S), 1) // S
    takes = [jnp.where(same, dot_nt(pick, stacked(rt, group)), 0.0).astype(BF16) for group in groups]

    toks = []
    for k, group in enumerate(groups):
        arrive((TOK, TOK2)[k], tk, len(group) - (k == 0))
        toks.append(stacked(tk, group))
        bs_[k] = dot(takes[k], toks[k]).astype(BF16).reshape(bs_.shape[1:])
        for p in cores:
            send((SLOT, SLOT2)[k], bs_.at[k, p], br.at[k, yc], (z * NC + p, t))
        br[k, yc] = bs_[k, yc]

    arrive(DENSE2, d3, NZ * (NC - 1) // NC)
    dense_w = d3[...].reshape(D, 128)
    pre = dot(jnp.concatenate(toks, axis=0), dense_w)
    act = silu(pltpu.roll(pre, 2 * hs, 1)) * pltpu.roll(pre, hs, 1)
    lane = iota(act.shape, 1)
    act = jnp.where(jnp.logical_and(lane >= 2 * hs, lane < 3 * hs), act, 0.0).astype(BF16)
    out = dot_nt(act, dense_w)
    for k in range(NZ):
        for j in range(NT):
            fs_[k * NT + j] = out[k * S : (k + 1) * S, j * quarter : (j + 1) * quarter].astype(BF16)
    for k in reversed(range(NZ)):
        for d in range(NT):
            if ring[k] or d:
                q = lax.rem(t + d, NT)
                send(DOUT, fs_.at[k * NT + q], fr.at[z * NT + t], (at[ring[k]] * NC + yc, q))
    fr[z * NT + t] = fs_[t]

    loads["g"].wait()
    loads["u"].wait()
    for k in range(2):
        arrive((SLOT, SLOT2)[k], br.at[k], NC - 1)
        arrived = br[k].reshape(rows_g, D)
        aa[k, t] = (silu(dot(arrived, vg[...])) * dot(arrived, vu[...])).astype(BF16)
        for p in ts:
            send((HID, HID2)[k], aa.at[k, t], aa.at[k, t], (e, p))

    arrive(DOWN, dq, NT - 1)
    down = jnp.concatenate([dq[k] for k in range(NT)], axis=0)
    for k, group in enumerate(groups):
        arrive((HID, HID2)[k], aa.at[k], NT - 1)
        hidden = jnp.concatenate([aa[k, j] for j in range(NT)], axis=1)
        gs_[k] = dot(hidden, down).astype(BF16).reshape(gs_.shape[1:])
        for i in reversed(range(half)):

            for j in range(0 if group[i] else 1, NC):
                send(RET, gs_.at[k, around[j] * half + i], gr.at[e], (at[group[i]] * NC + around[j], t))
    gr[e] = gs_[0, yc * half]

    arrive(DOUT, fr, NZ * NT - 1)
    dense = jnp.zeros((S, quarter), F32)
    for k in range(NZ * NT):
        dense = dense + fr[k].astype(F32)
    base = own + branch * dense
    arrive(RET, gr, NE - 1)
    mixed[...] = (base + dot(give.astype(BF16), gr[...].reshape(R, quarter))).astype(BF16)

    for i, ref, count in ((PART, pt, NT - 1), (ROUTE, rt, NZ - 1), (DENSE, d1, NZ - 1), (DENSE2, d3, NZ * (NC - 1) // NC), (DOWN, dq, NT - 1), (TOK, tk, NZ - 1), (SLOT, bs_.at[0], NC - 1), (SLOT2, bs_.at[1], NC - 1), (HID, aa.at[0], NT - 1), (HID2, aa.at[1], NT - 1), (RET, gr, NE - 1)):
        wait(ssem.at[i], ref, count)
    wait(ssem.at[DOUT], fr, NZ * NT - 1)


def store_kernel(count, *refs):
    ins, outs, sem = refs[:count], refs[count : 2 * count], refs[2 * count]
    copies = [pltpu.make_async_copy(a, b, sem.at[i]) for i, (a, b) in enumerate(zip(ins, outs))]
    for c in copies:
        c.start()
    for c in copies:
        c.wait()


def body(
    tokens, ssm_state, conv_x, conv_b, conv_c, w_x, w_z, w_b, w_c, w_dt, dt_bias, a_log, d_skip, taps_x, taps_b, taps_c,
    norm1_gain, group_gain, w_out, norm2_gain, route_ids, route_weights, exp_gate, exp_up, exp_down, dense_gate, dense_up, dense_down, branch_gate,
    *, NE, NC, NT, sd,
):
    S, D = tokens.shape
    NZ = NE // NC
    inner = w_x.shape[1]
    cols = w_b.shape[1]
    quarter = D // NT
    hidden = exp_gate.shape[2]
    R = 2 * NE
    rows = dense_gate.shape[0]
    vm, hbm, free = (pl.BlockSpec(memory_space=m) for m in (pltpu.VMEM, pltpu.HBM, pl.ANY))
    dma = pltpu.SemaphoreType.DMA
    half = lambda *shape: pltpu.VMEM(shape, BF16)
    shape = jax.ShapeDtypeStruct
    small = (
        tokens, turned(conv_x), turned(conv_b), turned(conv_c), w_dt.T, dt_bias[None], a_log[None], d_skip[None], taps_x, taps_b, taps_c, norm1_gain[None],
        group_gain[None], norm2_gain[None], route_ids, route_weights, dense_gate, dense_up, dense_down.T, branch_gate.reshape(D // 128, 128),
    )
    made = pl.pallas_call(
        functools.partial(step_kernel, NE, NC, NT, cols // sd),
        name="step",
        out_shape=(
            shape((S, quarter), BF16), shape(ssm_state.shape, F32), shape((3, S, inner), BF16), shape((3, S, cols), BF16), shape((3, S, cols), BF16),
        ),
        in_specs=[hbm] * 29,
        out_specs=(vm,) * 5,
        scratch_shapes=[pltpu.VMEM(a.shape, a.dtype) for a in small]
        + [
            half(D, inner), half(D, inner), half(D, cols), half(D, cols), pltpu.VMEM(ssm_state.shape, F32),
            half(inner, D), half(D, hidden), half(D, hidden), half(hidden, D),
            half(NT, S, D), half(NZ, rows, 128), half(NZ, rows, 128), half(NZ, NC, rows, 128), half(NT, hidden, quarter),
            half(NZ, S, D), half(NZ, S, R), half(2, NC, NZ, D), half(2, NC, NZ, D), half(2, NT, R // 2, hidden),
            half(NZ * NT, S, quarter), half(NZ * NT, S, quarter),
            half(2, NE // 2, 2, quarter), half(NE, 2, quarter),
            dma((8,)), dma((S,)), dma((20,)), dma((13,)), dma((13,)),
        ],
        compiler_params=pltpu.CompilerParams(collective_id=0, has_side_effects=True, vmem_limit_bytes=VMEM_STEP),
    )(
        *(fixed(a) for a in small),
        *(fixed(a) for a in (ssm_state, w_x, w_z, w_b, w_c, w_out, exp_gate, exp_up, exp_down)),
    )
    mixed, state_next, cx, cb, cc = pl.pallas_call(
        functools.partial(store_kernel, len(made)),
        name="store",
        out_shape=tuple(shape(a.shape, a.dtype) for a in made),
        in_specs=[free] * len(made),
        out_specs=(hbm,) * len(made),
        scratch_shapes=[dma((len(made),))],
        compiler_params=pltpu.CompilerParams(vmem_limit_bytes=VMEM_STORE),
    )(*made)
    return mixed, state_next, turned(cx), turned(cb), turned(cc)


def fixed(a):
    return pltpu.with_memory_space_constraint(a, pltpu.HBM)


def turned(a):
    return jnp.transpose(a, (1, 0, 2))


def solution(mesh):
    NT = mesh.shape["tp"]
    NC = 8 if mesh.shape["ep"] >= 64 else 2
    NE = mesh.shape["ep"]
    ep = P("ep", None)
    in_specs = (
        ep, P("ep", "tp", None, None), P("ep", None, "tp"), P("ep", None, "tp"), P("ep", None, "tp"),
        P(None, "tp"), P(None, "tp"), P(None, "tp"), P(None, "tp"), P(), P("tp"), P("tp"), P("tp"),
        P(None, "tp"), P(None, "tp"), P(None, "tp"), P(), P("tp"), P("tp", None), P(), ep, ep,
        P("ep", None, "tp"), P("ep", None, "tp"), P("ep", "tp", None), P("ep", "tp"), P("ep", "tp"), P("tp", "ep"), P(),
    )
    out_specs = (P("ep", "tp"), P("ep", "tp", None, None), P("ep", None, "tp"), P("ep", None, "tp"), P("ep", None, "tp"))
    part = functools.partial(body, NE=NE, NC=NC, NT=NT, sd=128)
    return jax.shard_map(part, mesh=mesh, in_specs=in_specs, out_specs=out_specs, check_vma=False)
```

```python
import functools

import jax
import jax.numpy as jnp
from jax import lax
from jax.experimental import pallas as pl
from jax.experimental.pallas import tpu as pltpu
from jax.sharding import PartitionSpec as P

EPS = 1e-06
F32 = jnp.float32
BF16 = jnp.bfloat16
HIGH = lax.Precision.HIGHEST
MESH = pl.DeviceIdType.MESH
VMEM_STEP = 24_000_000
VMEM_STORE = 4_000_000


def dot(a, b, **kw):
    return jnp.dot(a, b, preferred_element_type=F32, **kw)


def dot_nt(a, b, **kw):
    return lax.dot_general(a, b, (((1,), (1,)), ((), ())), preferred_element_type=F32, **kw)


def iota(shape, dim):
    return lax.broadcasted_iota(jnp.int32, shape, dim)


def rms_rows(values, gain):
    return values * lax.rsqrt(jnp.mean(values * values, axis=-1, keepdims=True) + EPS) * gain


def silu(v):
    return v * jax.nn.sigmoid(v)


def step_kernel(NE, NC, NT, n_groups, *refs):
    given, refs = refs[:20], refs[20:]
    state, w_x, w_z, w_b, w_c, w_out, w_g, w_u, w_d = refs[:9]
    mixed, state_out, cx_out, cb_out, cc_out = refs[9:14]
    small, refs = refs[14:34], refs[34:]
    tokens, conv_x, conv_b, conv_c, w_dt, dt_bias, a_log, d_skip, taps_x, taps_b, taps_c, gain = small[:12]
    ggain, gain2, ids, wts, dgate, dup, ddown, bgate = small[12:]
    vx, vz, vb, vc, st, vo, vg, vu, vd, pt, d1, d2, d3, dq, tk, rt, bs_, br, aa, fs_, fr, gs_, gr, lsem, isem, tsem, ssem, rsem = refs
    NZ = NE // NC
    S, D = tokens.shape
    heads, hd, sd = st.shape[1:]
    inner = heads * hd
    per = heads // n_groups
    quarter = D // NT
    R = 2 * NE
    e = lax.axis_index("ep")
    t = lax.axis_index("tp")
    z = e // NC
    yc = lax.rem(e, NC)

    ts = [lax.rem(t + d, NT) for d in range(1, NT)]
    ring = sorted(range(NZ), key=lambda d: (min(d, NZ - d), d))
    half = NZ // 2
    groups = (ring[:half], ring[half:])
    at = [lax.rem(z + d, NZ) for d in range(NZ)]
    zs = [at[d] for d in reversed(ring) if d]
    around = [lax.rem(yc + d, NC) for d in range(NC)]
    cores = around[1:]
    barrier = pltpu.get_barrier_semaphore()
    for dev in [(p * NC + yc, t) for p in zs] + [(z * NC + p, t) for p in cores] + [(e, p) for p in ts]:
        pl.semaphore_signal(barrier, inc=1, device_id=dev, device_id_type=MESH)

    loads = {}
    for i, (name, src, dst) in enumerate((
        ("x", w_x, vx), ("b", w_b, vb), ("c", w_c, vc), ("z", w_z, vz), ("o", w_out, vo), ("d", w_d.at[0], vd), ("g", w_g.at[0], vg), ("u", w_u.at[0], vu)
    )):
        loads[name] = pltpu.make_async_copy(src, dst, lsem.at[i])
    tiny = [pltpu.make_async_copy(src, dst, tsem.at[i]) for i, (src, dst) in enumerate(zip(given, small))]
    for c in tiny[:12]:
        c.start()
    for name in "xbcz":
        loads[name].start()
    ins = [pltpu.make_async_copy(state.at[s], st.at[s], isem.at[s]) for s in range(S)]
    for c in ins:
        c.start()
    loads["o"].start()
    for c in tiny[12:]:
        c.start()
    for name in "dgu":
        loads[name].start()

    PART, ROUTE, DENSE, DENSE2, DOWN, TOK, SLOT, DOUT, HID, RET, TOK2, SLOT2, HID2 = range(13)

    def send(i, src, dst, dev, there=None):
        pltpu.make_async_remote_copy(src_ref=src, dst_ref=dst, send_sem=ssem.at[i], recv_sem=rsem.at[i if there is None else there], device_id=dev, device_id_type=MESH).start()

    def wait(sem, ref, count):
        pltpu.make_async_copy(ref.at[pl.ds(0, count)], ref.at[pl.ds(0, count)], sem).wait()

    def arrive(i, ref, count):
        wait(rsem.at[i], ref, count)

    for c in tiny[:12]:
        c.wait()
    normed = rms_rows(tokens[...].astype(F32), gain[...]).astype(BF16)
    raw = dot_nt(normed, w_dt[...])
    total_heads = raw.shape[1]
    spread_all = (iota((total_heads, inner), 0) == t * heads + iota((total_heads, inner), 1) // hd).astype(F32)
    spread = (iota((heads, inner), 0) == iota((heads, inner), 1) // hd).astype(F32)
    raw = dot(raw, spread_all, precision=HIGH)
    bias = dot(dt_bias[...], spread, precision=HIGH)
    rate = jnp.exp(dot(a_log[...], spread, precision=HIGH))
    skip = dot(d_skip[...], spread, precision=HIGH)
    pre = raw + bias
    step = jnp.maximum(pre, 0.0) + jnp.log1p(jnp.exp(-jnp.abs(pre)))
    decay = jnp.exp(-step * rate)

    def conv(prev, fresh, taps, out):
        fresh = fresh.astype(BF16)
        tap = taps[...].astype(F32)
        depth = prev.shape[0]
        total = fresh.astype(F32) * tap[depth : depth + 1]
        for j in range(depth):
            total = total + prev[j].astype(F32) * tap[j : j + 1]
            out[j] = prev[j + 1] if j + 1 < depth else fresh
        return silu(total)

    for name in "xbc":
        loads[name].wait()
    xs = conv(conv_x, dot(normed, vx[...]), taps_x, cx_out)
    bs = conv(conv_b, dot(normed, vb[...]), taps_b, cb_out)
    cs = conv(conv_c, dot(normed, vc[...]), taps_c, cc_out)
    inflow = step * xs
    rows = per * hd
    loads["z"].wait()
    lane = iota((rows, S), 1)
    reads = [jnp.zeros((rows, S), F32) for _ in range(n_groups)]
    for s in range(S):
        if s % 4 == 0:
            for c in ins[s : s + 4]:
                c.wait()
        if s == 0:
            zz = dot(normed, vz[...]).astype(BF16).astype(F32)
        for g in range(n_groups):
            old = st[s, g * per : (g + 1) * per].reshape(rows, sd)
            got = jnp.sum(old * cs[s : s + 1, g * sd : (g + 1) * sd], axis=1, keepdims=True)
            reads[g] = jnp.where(lane == s, got, reads[g])
    both = [jnp.sum(bs[:, g * sd : (g + 1) * sd] * cs[:, g * sd : (g + 1) * sd], axis=1, keepdims=True) for g in range(n_groups)]
    for c in tiny[12:]:
        c.wait()
    parts = []
    for g in range(n_groups):
        cut = slice(g * rows, (g + 1) * rows)
        v = decay[:, cut] * reads[g].T + inflow[:, cut] * both[g] + skip[:, cut] * xs[:, cut]
        v = v * silu(zz[:, cut])
        parts.append(v * lax.rsqrt(jnp.mean(v * v, axis=-1, keepdims=True) + EPS) * ggain[:, cut])
    mixed_heads = jnp.concatenate(parts, axis=1).astype(BF16)
    loads["o"].wait()
    pt[t] = dot(mixed_heads, vo[...]).astype(BF16)

    pl.semaphore_wait(barrier, (NZ - 1) + (NC - 1) + (NT - 1))
    for p in ts:
        send(PART, pt.at[t], pt.at[t], (e, p))

    slot = iota((S, R), 1)
    named = jnp.zeros((S, R), F32)
    weight = jnp.zeros((S, R), F32)
    for k in range(ids.shape[1]):
        hit = ids[:, k : k + 1] == slot // 2
        named = jnp.where(hit, 1.0, named)
        weight = jnp.where(hit, wts[:, k : k + 1], weight)
    before = (iota((S, S), 0) > iota((S, S), 1)).astype(F32)
    rank = dot(before, named)
    mine = jnp.logical_and(named > 0.5, jnp.abs(rank - lax.rem(slot, 2).astype(F32)) < 0.5)
    rt[z] = jnp.where(mine, 1.0, 0.0).astype(BF16)
    give = jnp.where(mine, weight, 0.0)
    hs = dgate.shape[1] // NZ
    lane = iota((dgate.shape[0], 128), 1)
    three = [dgate[...].astype(F32), dup[...].astype(F32), ddown[...].astype(F32)]
    for k in range(NZ):
        page, off = k * hs // 128 * 128, k * hs % 128
        block = jnp.zeros(lane.shape, F32)
        for j, v in enumerate(three):
            v = v[:, page : page + 128]
            shift = (j * hs - off) % 128
            block = jnp.where(jnp.logical_and(lane >= j * hs, lane < (j + 1) * hs), pltpu.roll(v, shift, 1) if shift else v, block)
        d1[k] = block.astype(BF16)
    for p in zs:
        send(ROUTE, rt.at[z], rt.at[z], (p * NC + yc, t))
        send(DENSE, d1.at[p], d2.at[z], (p * NC + yc, t))
    d2[z] = d1[z]
    loads["d"].wait()

    in_col = inflow.T
    decay_col = decay.T
    for s in range(S):
        for g in range(n_groups):
            cut = slice(g * rows, (g + 1) * rows)
            old = st[s, g * per : (g + 1) * per].reshape(rows, sd)
            new = decay_col[cut, s : s + 1] * old + in_col[cut, s : s + 1] * bs[s : s + 1, g * sd : (g + 1) * sd]
            state_out[s, g * per : (g + 1) * per] = new.reshape(per, hd, sd)

    arrive(PART, pt, NT - 1)
    total = pt[0].astype(F32)
    for k in range(1, NT):
        total = total + pt[k].astype(F32)
    residual = (tokens[...].astype(F32) + total).astype(BF16).astype(F32)
    normed2 = rms_rows(residual, gain2[...]).astype(BF16)
    tk[z] = normed2
    for d in reversed(ring[1:]):
        send(TOK, tk.at[z], tk.at[z], (at[d] * NC + yc, t), TOK2 if (NZ - d) % NZ in groups[1] else TOK)

    for p in ts:
        send(DOWN, vd.at[:, pl.ds(pl.multiple_of(p * quarter, quarter), quarter)], dq.at[t], (e, p))
    dq[t] = vd[:, pl.ds(pl.multiple_of(t * quarter, quarter), quarter)]

    arrive(DENSE, d2, NZ - 1)
    for p in cores:
        send(DENSE2, d2, d3.at[:, yc], (z * NC + p, t))
    for k in range(NZ):
        d3[k, yc] = d2[k]

    lanes = bgate.shape[1]
    weighted = jnp.zeros((S, lanes), F32)
    for k in range(bgate.shape[0]):
        weighted = weighted + normed2[:, k * lanes : (k + 1) * lanes].astype(F32) * bgate[k : k + 1, :].astype(F32)
    branch = jax.nn.sigmoid(jnp.sum(weighted, axis=1, keepdims=True))
    own = jnp.zeros((S, quarter), F32)
    for k in range(NT):
        own = jnp.where(t == k, residual[:, k * quarter : (k + 1) * quarter], own)

    def stacked(ref, offsets):
        return jnp.concatenate([ref[at[d]].astype(F32) for d in offsets], axis=0).astype(BF16)

    arrive(ROUTE, rt, NZ - 1)
    rows_g = NC * half * 2
    row, col = iota((rows_g, R), 0), iota((rows_g, R), 1)
    pick = (col == z * 2 * NC + 2 * (row // (2 * half)) + lax.rem(row, 2)).astype(BF16)
    same = lax.rem(iota((rows_g, half * S), 0) // 2, half) == iota((rows_g, half * S), 1) // S
    takes = [jnp.where(same, dot_nt(pick, stacked(rt, group)), 0.0).astype(BF16) for group in groups]

    toks = []
    for k, group in enumerate(groups):
        arrive((TOK, TOK2)[k], tk, len(group) - (k == 0))
        toks.append(stacked(tk, group))
        bs_[k] = dot(takes[k], toks[k]).astype(BF16).reshape(bs_.shape[1:])
        for p in cores:
            send((SLOT, SLOT2)[k], bs_.at[k, p], br.at[k, yc], (z * NC + p, t))
        br[k, yc] = bs_[k, yc]

    arrive(DENSE2, d3, NZ * (NC - 1) // NC)
    dense_w = d3[...].reshape(D, 128)
    pre = dot(jnp.concatenate(toks, axis=0), dense_w)
    act = silu(pltpu.roll(pre, 2 * hs, 1)) * pltpu.roll(pre, hs, 1)
    lane = iota(act.shape, 1)
    act = jnp.where(jnp.logical_and(lane >= 2 * hs, lane < 3 * hs), act, 0.0).astype(BF16)
    out = dot_nt(act, dense_w)
    for k in range(NZ):
        for j in range(NT):
            fs_[k * NT + j] = out[k * S : (k + 1) * S, j * quarter : (j + 1) * quarter].astype(BF16)
    for k in reversed(range(NZ)):
        for d in range(NT):
            if ring[k] or d:
                q = lax.rem(t + d, NT)
                send(DOUT, fs_.at[k * NT + q], fr.at[z * NT + t], (at[ring[k]] * NC + yc, q))
    fr[z * NT + t] = fs_[t]

    loads["g"].wait()
    loads["u"].wait()
    for k in range(2):
        arrive((SLOT, SLOT2)[k], br.at[k], NC - 1)
        arrived = br[k].reshape(rows_g, D)
        aa[k, t] = (silu(dot(arrived, vg[...])) * dot(arrived, vu[...])).astype(BF16)
        for p in ts:
            send((HID, HID2)[k], aa.at[k, t], aa.at[k, t], (e, p))

    arrive(DOWN, dq, NT - 1)
    down = jnp.concatenate([dq[k] for k in range(NT)], axis=0)
    for k, group in enumerate(groups):
        arrive((HID, HID2)[k], aa.at[k], NT - 1)
        hidden = jnp.concatenate([aa[k, j] for j in range(NT)], axis=1)
        gs_[k] = dot(hidden, down).astype(BF16).reshape(gs_.shape[1:])
        for i in reversed(range(half)):

            for j in range(0 if group[i] else 1, NC):
                send(RET, gs_.at[k, around[j] * half + i], gr.at[e], (at[group[i]] * NC + around[j], t))
    gr[e] = gs_[0, yc * half]

    arrive(DOUT, fr, NZ * NT - 1)
    dense = jnp.zeros((S, quarter), F32)
    for k in range(NZ * NT):
        dense = dense + fr[k].astype(F32)
    base = own + branch * dense
    arrive(RET, gr, NE - 1)
    mixed[...] = (base + dot(give.astype(BF16), gr[...].reshape(R, quarter))).astype(BF16)

    for i, ref, count in ((PART, pt, NT - 1), (ROUTE, rt, NZ - 1), (DENSE, d1, NZ - 1), (DENSE2, d3, NZ * (NC - 1) // NC), (DOWN, dq, NT - 1), (TOK, tk, NZ - 1), (SLOT, bs_.at[0], NC - 1), (SLOT2, bs_.at[1], NC - 1), (HID, aa.at[0], NT - 1), (HID2, aa.at[1], NT - 1), (RET, gr, NE - 1)):
        wait(ssem.at[i], ref, count)
    wait(ssem.at[DOUT], fr, NZ * NT - 1)


def store_kernel(count, *refs):
    ins, outs, sem = refs[:count], refs[count : 2 * count], refs[2 * count]
    copies = [pltpu.make_async_copy(a, b, sem.at[i]) for i, (a, b) in enumerate(zip(ins, outs))]
    for c in copies:
        c.start()
    for c in copies:
        c.wait()


def body(
    tokens, ssm_state, conv_x, conv_b, conv_c, w_x, w_z, w_b, w_c, w_dt, dt_bias, a_log, d_skip, taps_x, taps_b, taps_c,
    norm1_gain, group_gain, w_out, norm2_gain, route_ids, route_weights, exp_gate, exp_up, exp_down, dense_gate, dense_up, dense_down, branch_gate,
    *, NE, NC, NT, sd,
):
    S, D = tokens.shape
    NZ = NE // NC
    inner = w_x.shape[1]
    cols = w_b.shape[1]
    quarter = D // NT
    hidden = exp_gate.shape[2]
    R = 2 * NE
    rows = dense_gate.shape[0]
    vm, hbm, free = (pl.BlockSpec(memory_space=m) for m in (pltpu.VMEM, pltpu.HBM, pl.ANY))
    dma = pltpu.SemaphoreType.DMA
    half = lambda *shape: pltpu.VMEM(shape, BF16)
    shape = jax.ShapeDtypeStruct
    small = (
        tokens, turned(conv_x), turned(conv_b), turned(conv_c), w_dt.T, dt_bias[None], a_log[None], d_skip[None], taps_x, taps_b, taps_c, norm1_gain[None],
        group_gain[None], norm2_gain[None], route_ids, route_weights, dense_gate, dense_up, dense_down.T, branch_gate.reshape(D // 128, 128),
    )
    made = pl.pallas_call(
        functools.partial(step_kernel, NE, NC, NT, cols // sd),
        name="step",
        out_shape=(
            shape((S, quarter), BF16), shape(ssm_state.shape, F32), shape((3, S, inner), BF16), shape((3, S, cols), BF16), shape((3, S, cols), BF16),
        ),
        in_specs=[hbm] * 29,
        out_specs=(vm,) * 5,
        scratch_shapes=[pltpu.VMEM(a.shape, a.dtype) for a in small]
        + [
            half(D, inner), half(D, inner), half(D, cols), half(D, cols), pltpu.VMEM(ssm_state.shape, F32),
            half(inner, D), half(D, hidden), half(D, hidden), half(hidden, D),
            half(NT, S, D), half(NZ, rows, 128), half(NZ, rows, 128), half(NZ, NC, rows, 128), half(NT, hidden, quarter),
            half(NZ, S, D), half(NZ, S, R), half(2, NC, NZ, D), half(2, NC, NZ, D), half(2, NT, R // 2, hidden),
            half(NZ * NT, S, quarter), half(NZ * NT, S, quarter),
            half(2, NE // 2, 2, quarter), half(NE, 2, quarter),
            dma((8,)), dma((S,)), dma((20,)), dma((13,)), dma((13,)),
        ],
        compiler_params=pltpu.CompilerParams(collective_id=0, has_side_effects=True, vmem_limit_bytes=VMEM_STEP),
    )(
        *(fixed(a) for a in small),
        *(fixed(a) for a in (ssm_state, w_x, w_z, w_b, w_c, w_out, exp_gate, exp_up, exp_down)),
    )
    mixed, state_next, cx, cb, cc = pl.pallas_call(
        functools.partial(store_kernel, len(made)),
        name="store",
        out_shape=tuple(shape(a.shape, a.dtype) for a in made),
        in_specs=[free] * len(made),
        out_specs=(hbm,) * len(made),
        scratch_shapes=[dma((len(made),))],
        compiler_params=pltpu.CompilerParams(vmem_limit_bytes=VMEM_STORE),
    )(*made)
    return mixed, state_next, turned(cx), turned(cb), turned(cc)


def fixed(a):
    return pltpu.with_memory_space_constraint(a, pltpu.HBM)


def turned(a):
    return jnp.transpose(a, (1, 0, 2))


def solution(mesh):
    NT = mesh.shape["tp"]
    NC = 8 if mesh.shape["ep"] >= 64 else 2
    NE = mesh.shape["ep"]
    ep = P("ep", None)
    in_specs = (
        ep, P("ep", "tp", None, None), P("ep", None, "tp"), P("ep", None, "tp"), P("ep", None, "tp"),
        P(None, "tp"), P(None, "tp"), P(None, "tp"), P(None, "tp"), P(), P("tp"), P("tp"), P("tp"),
        P(None, "tp"), P(None, "tp"), P(None, "tp"), P(), P("tp"), P("tp", None), P(), ep, ep,
        P("ep", None, "tp"), P("ep", None, "tp"), P("ep", "tp", None), P("ep", "tp"), P("ep", "tp"), P("tp", "ep"), P(),
    )
    out_specs = (P("ep", "tp"), P("ep", "tp", None, None), P("ep", None, "tp"), P("ep", None, "tp"), P("ep", None, "tp"))
    part = functools.partial(body, NE=NE, NC=NC, NT=NT, sd=128)
    return jax.shard_map(part, mesh=mesh, in_specs=in_specs, out_specs=out_specs, check_vma=False)
```

```python
import functools

import jax
import jax.numpy as jnp
from jax import lax
from jax.experimental import pallas as pl
from jax.experimental.pallas import tpu as pltpu
from jax.sharding import PartitionSpec as P

EPS = 1e-06
F32 = jnp.float32
BF16 = jnp.bfloat16
HIGH = lax.Precision.HIGHEST
MESH = pl.DeviceIdType.MESH
VMEM_STEP = 24_000_000
VMEM_STORE = 4_000_000


def dot(a, b, **kw):
    return jnp.dot(a, b, preferred_element_type=F32, **kw)


def dot_nt(a, b, **kw):
    return lax.dot_general(a, b, (((1,), (1,)), ((), ())), preferred_element_type=F32, **kw)


def iota(shape, dim):
    return lax.broadcasted_iota(jnp.int32, shape, dim)


def rms_rows(values, gain):
    return values * lax.rsqrt(jnp.mean(values * values, axis=-1, keepdims=True) + EPS) * gain


def silu(v):
    return v * jax.nn.sigmoid(v)


def step_kernel(NE, NC, NT, n_groups, *refs):
    given, refs = refs[:20], refs[20:]
    state, w_x, w_z, w_b, w_c, w_out, w_g, w_u, w_d = refs[:9]
    mixed, state_out, cx_out, cb_out, cc_out = refs[9:14]
    small, refs = refs[14:34], refs[34:]
    tokens, conv_x, conv_b, conv_c, w_dt, dt_bias, a_log, d_skip, taps_x, taps_b, taps_c, gain = small[:12]
    ggain, gain2, ids, wts, dgate, dup, ddown, bgate = small[12:]
    vx, vz, vb, vc, st, vo, vg, vu, vd, pt, d1, d2, d3, dq, tk, rt, bs_, br, aa, fs_, fx, fz, fr, gs_, gr, lsem, isem, tsem, ssem, rsem = refs
    NZ = NE // NC
    S, D = tokens.shape
    heads, hd, sd = st.shape[1:]
    inner = heads * hd
    per = heads // n_groups
    quarter = D // NT
    R = 2 * NE
    e = lax.axis_index("ep")
    t = lax.axis_index("tp")
    z = e // NC
    yc = lax.rem(e, NC)

    ts = [lax.rem(t + d, NT) for d in range(1, NT)]
    ring = sorted(range(NZ), key=lambda d: (min(d, NZ - d), d))
    half = NZ // 2
    groups = (ring[:half], ring[half:])
    at = [lax.rem(z + d, NZ) for d in range(NZ)]
    zs = [at[d] for d in reversed(ring) if d]
    around = [lax.rem(yc + d, NC) for d in range(NC)]
    cores = around[1:]
    barrier = pltpu.get_barrier_semaphore()
    for dev in [(p * NC + yc, t) for p in zs] + [(z * NC + p, t) for p in cores] + [(e, p) for p in ts]:
        pl.semaphore_signal(barrier, inc=1, device_id=dev, device_id_type=MESH)

    loads = {}
    for i, (name, src, dst) in enumerate((
        ("x", w_x, vx), ("b", w_b, vb), ("c", w_c, vc), ("z", w_z, vz), ("o", w_out, vo), ("d", w_d.at[0], vd), ("g", w_g.at[0], vg), ("u", w_u.at[0], vu)
    )):
        loads[name] = pltpu.make_async_copy(src, dst, lsem.at[i])
    tiny = [pltpu.make_async_copy(src, dst, tsem.at[i]) for i, (src, dst) in enumerate(zip(given, small))]
    for c in tiny[:12]:
        c.start()
    for name in "xbc":
        loads[name].start()
    for c in tiny[12:]:
        c.start()
    loads["z"].start()
    ins = [pltpu.make_async_copy(state.at[s], st.at[s], isem.at[s]) for s in range(S)]
    for c in ins:
        c.start()
    loads["o"].start()
    for name in "dgu":
        loads[name].start()

    PART, ROUTE, DENSE, DENSE2, DOWN, TOK, SLOT, DOUT, HID, RET, TOK2, SLOT2, HID2, DZ = range(14)

    def send(i, src, dst, dev, there=None):
        pltpu.make_async_remote_copy(src_ref=src, dst_ref=dst, send_sem=ssem.at[i], recv_sem=rsem.at[i if there is None else there], device_id=dev, device_id_type=MESH).start()

    def wait(sem, ref, count):
        pltpu.make_async_copy(ref.at[pl.ds(0, count)], ref.at[pl.ds(0, count)], sem).wait()

    def arrive(i, ref, count):
        wait(rsem.at[i], ref, count)

    for c in tiny[:12]:
        c.wait()
    normed = rms_rows(tokens[...].astype(F32), gain[...]).astype(BF16)
    raw = dot_nt(normed, w_dt[...])
    total_heads = raw.shape[1]
    spread_all = (iota((total_heads, inner), 0) == t * heads + iota((total_heads, inner), 1) // hd).astype(F32)
    spread = (iota((heads, inner), 0) == iota((heads, inner), 1) // hd).astype(F32)
    raw = dot(raw, spread_all, precision=HIGH)
    bias = dot(dt_bias[...], spread, precision=HIGH)
    rate = jnp.exp(dot(a_log[...], spread, precision=HIGH))
    skip = dot(d_skip[...], spread, precision=HIGH)
    pre = raw + bias
    step = jnp.maximum(pre, 0.0) + jnp.log1p(jnp.exp(-jnp.abs(pre)))
    decay = jnp.exp(-step * rate)

    def conv(prev, fresh, taps, out):
        fresh = fresh.astype(BF16)
        tap = taps[...].astype(F32)
        depth = prev.shape[0]
        total = fresh.astype(F32) * tap[depth : depth + 1]
        for j in range(depth):
            total = total + prev[j].astype(F32) * tap[j : j + 1]
            out[j] = prev[j + 1] if j + 1 < depth else fresh
        return silu(total)

    for name in "xbc":
        loads[name].wait()
    xs = conv(conv_x, dot(normed, vx[...]), taps_x, cx_out)
    bs = conv(conv_b, dot(normed, vb[...]), taps_b, cb_out)
    cs = conv(conv_c, dot(normed, vc[...]), taps_c, cc_out)
    inflow = step * xs
    for c in tiny[12:]:
        c.wait()
    slot = iota((S, R), 1)
    named = jnp.zeros((S, R), F32)
    weight = jnp.zeros((S, R), F32)
    for k in range(ids.shape[1]):
        hit = ids[:, k : k + 1] == slot // 2
        named = jnp.where(hit, 1.0, named)
        weight = jnp.where(hit, wts[:, k : k + 1], weight)
    before = (iota((S, S), 0) > iota((S, S), 1)).astype(F32)
    rank = dot(before, named)
    mine = jnp.logical_and(named > 0.5, jnp.abs(rank - lax.rem(slot, 2).astype(F32)) < 0.5)
    rt[z] = jnp.where(mine, 1.0, 0.0).astype(BF16)
    give = jnp.where(mine, weight, 0.0)
    hs = dgate.shape[1] // NZ
    lane = iota((dgate.shape[0], 128), 1)
    three = [dgate[...].astype(F32), dup[...].astype(F32), ddown[...].astype(F32)]
    for k in range(NZ):
        page, off = k * hs // 128 * 128, k * hs % 128
        block = jnp.zeros(lane.shape, F32)
        for j, v in enumerate(three):
            v = v[:, page : page + 128]
            shift = (j * hs - off) % 128
            block = jnp.where(jnp.logical_and(lane >= j * hs, lane < (j + 1) * hs), pltpu.roll(v, shift, 1) if shift else v, block)
        d1[k] = block.astype(BF16)
    pl.semaphore_wait(barrier, (NZ - 1) + (NC - 1) + (NT - 1))
    for p in zs:
        send(ROUTE, rt.at[z], rt.at[z], (p * NC + yc, t))
        send(DENSE, d1.at[p], d2.at[z], (p * NC + yc, t))
    d2[z] = d1[z]

    rows = per * hd
    loads["z"].wait()
    lane = iota((rows, S), 1)
    reads = [jnp.zeros((rows, S), F32) for _ in range(n_groups)]
    for s in range(S):
        if s % 4 == 0:
            for c in ins[s : s + 4]:
                c.wait()
        if s == 0:
            zz = dot(normed, vz[...]).astype(BF16).astype(F32)
        for g in range(n_groups):
            old = st[s, g * per : (g + 1) * per].reshape(rows, sd)
            got = jnp.sum(old * cs[s : s + 1, g * sd : (g + 1) * sd], axis=1, keepdims=True)
            reads[g] = jnp.where(lane == s, got, reads[g])
    both = [jnp.sum(bs[:, g * sd : (g + 1) * sd] * cs[:, g * sd : (g + 1) * sd], axis=1, keepdims=True) for g in range(n_groups)]
    parts = []
    for g in range(n_groups):
        cut = slice(g * rows, (g + 1) * rows)
        v = decay[:, cut] * reads[g].T + inflow[:, cut] * both[g] + skip[:, cut] * xs[:, cut]
        v = v * silu(zz[:, cut])
        parts.append(v * lax.rsqrt(jnp.mean(v * v, axis=-1, keepdims=True) + EPS) * ggain[:, cut])
    mixed_heads = jnp.concatenate(parts, axis=1).astype(BF16)
    loads["o"].wait()
    pt[t] = dot(mixed_heads, vo[...]).astype(BF16)

    for p in ts:
        send(PART, pt.at[t], pt.at[t], (e, p))

    loads["d"].wait()

    in_col = inflow.T
    decay_col = decay.T
    for s in range(S):
        for g in range(n_groups):
            cut = slice(g * rows, (g + 1) * rows)
            old = st[s, g * per : (g + 1) * per].reshape(rows, sd)
            new = decay_col[cut, s : s + 1] * old + in_col[cut, s : s + 1] * bs[s : s + 1, g * sd : (g + 1) * sd]
            state_out[s, g * per : (g + 1) * per] = new.reshape(per, hd, sd)

    arrive(DENSE, d2, NZ - 1)
    for p in cores:
        send(DENSE2, d2, d3.at[:, yc], (z * NC + p, t))
    for k in range(NZ):
        d3[k, yc] = d2[k]

    arrive(PART, pt, NT - 1)
    total = pt[0].astype(F32)
    for k in range(1, NT):
        total = total + pt[k].astype(F32)
    residual = (tokens[...].astype(F32) + total).astype(BF16).astype(F32)
    normed2 = rms_rows(residual, gain2[...]).astype(BF16)
    tk[z] = normed2
    for d in reversed(ring[1:]):
        send(TOK, tk.at[z], tk.at[z], (at[d] * NC + yc, t), TOK2 if (NZ - d) % NZ in groups[1] else TOK)

    for p in ts:
        send(DOWN, vd.at[:, pl.ds(pl.multiple_of(p * quarter, quarter), quarter)], dq.at[t], (e, p))
    dq[t] = vd[:, pl.ds(pl.multiple_of(t * quarter, quarter), quarter)]

    lanes = bgate.shape[1]
    weighted = jnp.zeros((S, lanes), F32)
    for k in range(bgate.shape[0]):
        weighted = weighted + normed2[:, k * lanes : (k + 1) * lanes].astype(F32) * bgate[k : k + 1, :].astype(F32)
    branch = jax.nn.sigmoid(jnp.sum(weighted, axis=1, keepdims=True))
    own = jnp.zeros((S, quarter), F32)
    for k in range(NT):
        own = jnp.where(t == k, residual[:, k * quarter : (k + 1) * quarter], own)

    def stacked(ref, offsets):
        return jnp.concatenate([ref[at[d]].astype(F32) for d in offsets], axis=0).astype(BF16)

    arrive(ROUTE, rt, NZ - 1)
    rows_g = NC * half * 2
    row, col = iota((rows_g, R), 0), iota((rows_g, R), 1)
    pick = (col == z * 2 * NC + 2 * (row // (2 * half)) + lax.rem(row, 2)).astype(BF16)
    same = lax.rem(iota((rows_g, half * S), 0) // 2, half) == iota((rows_g, half * S), 1) // S
    takes = [jnp.where(same, dot_nt(pick, stacked(rt, group)), 0.0).astype(BF16) for group in groups]

    toks = []
    for k, group in enumerate(groups):
        arrive((TOK, TOK2)[k], tk, len(group) - (k == 0))
        toks.append(stacked(tk, group))
        bs_[k] = dot(takes[k], toks[k]).astype(BF16).reshape(bs_.shape[1:])
        for p in cores:
            send((SLOT, SLOT2)[k], bs_.at[k, p], br.at[k, yc], (z * NC + p, t))
        br[k, yc] = bs_[k, yc]

    arrive(DENSE2, d3, NZ * (NC - 1) // NC)
    dense_w = d3[...].reshape(D, 128)
    pre = dot(jnp.concatenate(toks, axis=0), dense_w)
    act = silu(pltpu.roll(pre, 2 * hs, 1)) * pltpu.roll(pre, hs, 1)
    lane = iota(act.shape, 1)
    act = jnp.where(jnp.logical_and(lane >= 2 * hs, lane < 3 * hs), act, 0.0).astype(BF16)
    out = dot_nt(act, dense_w)
    for k in range(NZ):
        for j in range(NT):
            fs_[j, k] = out[k * S : (k + 1) * S, j * quarter : (j + 1) * quarter].astype(BF16)
    for p in ts:
        send(DOUT, fs_.at[p], fx.at[t], (e, p))
    fx[t] = fs_[t]

    loads["g"].wait()
    loads["u"].wait()
    for k in range(2):
        arrive((SLOT, SLOT2)[k], br.at[k], NC - 1)
        arrived = br[k].reshape(rows_g, D)
        aa[k, t] = (silu(dot(arrived, vg[...])) * dot(arrived, vu[...])).astype(BF16)
        for p in ts:
            send((HID, HID2)[k], aa.at[k, t], aa.at[k, t], (e, p))

    arrive(DOUT, fx, NT - 1)
    for k in range(NZ):
        v = fx[0, k].astype(F32)
        for j in range(1, NT):
            v = v + fx[j, k].astype(F32)
        fz[k] = v.astype(BF16)
    for k in reversed(range(1, NZ)):
        send(DZ, fz.at[k], fr.at[z], (at[ring[k]] * NC + yc, t))
    fr[z] = fz[0]

    arrive(DOWN, dq, NT - 1)
    down = jnp.concatenate([dq[k] for k in range(NT)], axis=0)
    for k, group in enumerate(groups):
        arrive((HID, HID2)[k], aa.at[k], NT - 1)
        hidden = jnp.concatenate([aa[k, j] for j in range(NT)], axis=1)
        gs_[k] = dot(hidden, down).astype(BF16).reshape(gs_.shape[1:])
        for i in reversed(range(half)):

            for j in range(0 if group[i] else 1, NC):
                send(RET, gs_.at[k, around[j] * half + i], gr.at[e], (at[group[i]] * NC + around[j], t))
    gr[e] = gs_[0, yc * half]

    arrive(DZ, fr, NZ - 1)
    dense = jnp.zeros((S, quarter), F32)
    for k in range(NZ):
        dense = dense + fr[k].astype(F32)
    base = own + branch * dense
    arrive(RET, gr, NE - 1)
    mixed[...] = (base + dot(give.astype(BF16), gr[...].reshape(R, quarter))).astype(BF16)

    for i, ref, count in ((PART, pt, NT - 1), (ROUTE, rt, NZ - 1), (DENSE, d1, NZ - 1), (DENSE2, d3, NZ * (NC - 1) // NC), (DOWN, dq, NT - 1), (TOK, tk, NZ - 1), (SLOT, bs_.at[0], NC - 1), (SLOT2, bs_.at[1], NC - 1), (HID, aa.at[0], NT - 1), (HID2, aa.at[1], NT - 1), (RET, gr, NE - 1)):
        wait(ssem.at[i], ref, count)
    wait(ssem.at[DOUT], fx, NT - 1)
    wait(ssem.at[DZ], fr, NZ - 1)


def store_kernel(count, *refs):
    ins, outs, sem = refs[:count], refs[count : 2 * count], refs[2 * count]
    copies = [pltpu.make_async_copy(a, b, sem.at[i]) for i, (a, b) in enumerate(zip(ins, outs))]
    for c in copies:
        c.start()
    for c in copies:
        c.wait()


def body(
    tokens, ssm_state, conv_x, conv_b, conv_c, w_x, w_z, w_b, w_c, w_dt, dt_bias, a_log, d_skip, taps_x, taps_b, taps_c,
    norm1_gain, group_gain, w_out, norm2_gain, route_ids, route_weights, exp_gate, exp_up, exp_down, dense_gate, dense_up, dense_down, branch_gate,
    *, NE, NC, NT, sd,
):
    S, D = tokens.shape
    NZ = NE // NC
    inner = w_x.shape[1]
    cols = w_b.shape[1]
    quarter = D // NT
    hidden = exp_gate.shape[2]
    R = 2 * NE
    rows = dense_gate.shape[0]
    vm, hbm, free = (pl.BlockSpec(memory_space=m) for m in (pltpu.VMEM, pltpu.HBM, pl.ANY))
    dma = pltpu.SemaphoreType.DMA
    half = lambda *shape: pltpu.VMEM(shape, BF16)
    shape = jax.ShapeDtypeStruct
    small = (
        tokens, turned(conv_x), turned(conv_b), turned(conv_c), w_dt.T, dt_bias[None], a_log[None], d_skip[None], taps_x, taps_b, taps_c, norm1_gain[None],
        group_gain[None], norm2_gain[None], route_ids, route_weights, dense_gate, dense_up, dense_down.T, branch_gate.reshape(D // 128, 128),
    )
    made = pl.pallas_call(
        functools.partial(step_kernel, NE, NC, NT, cols // sd),
        name="step",
        out_shape=(
            shape((S, quarter), BF16), shape(ssm_state.shape, F32), shape((3, S, inner), BF16), shape((3, S, cols), BF16), shape((3, S, cols), BF16),
        ),
        in_specs=[hbm] * 29,
        out_specs=(vm,) * 5,
        scratch_shapes=[pltpu.VMEM(a.shape, a.dtype) for a in small]
        + [
            half(D, inner), half(D, inner), half(D, cols), half(D, cols), pltpu.VMEM(ssm_state.shape, F32),
            half(inner, D), half(D, hidden), half(D, hidden), half(hidden, D),
            half(NT, S, D), half(NZ, rows, 128), half(NZ, rows, 128), half(NZ, NC, rows, 128), half(NT, hidden, quarter),
            half(NZ, S, D), half(NZ, S, R), half(2, NC, NZ, D), half(2, NC, NZ, D), half(2, NT, R // 2, hidden),
            half(NT, NZ, S, quarter), half(NT, NZ, S, quarter), half(NZ, S, quarter), half(NZ, S, quarter),
            half(2, NE // 2, 2, quarter), half(NE, 2, quarter),
            dma((8,)), dma((S,)), dma((20,)), dma((14,)), dma((14,)),
        ],
        compiler_params=pltpu.CompilerParams(collective_id=0, has_side_effects=True, vmem_limit_bytes=VMEM_STEP),
    )(
        *(fixed(a) for a in small),
        *(fixed(a) for a in (ssm_state, w_x, w_z, w_b, w_c, w_out, exp_gate, exp_up, exp_down)),
    )
    mixed, state_next, cx, cb, cc = pl.pallas_call(
        functools.partial(store_kernel, len(made)),
        name="store",
        out_shape=tuple(shape(a.shape, a.dtype) for a in made),
        in_specs=[free] * len(made),
        out_specs=(hbm,) * len(made),
        scratch_shapes=[dma((len(made),))],
        compiler_params=pltpu.CompilerParams(vmem_limit_bytes=VMEM_STORE),
    )(*made)
    return mixed, state_next, turned(cx), turned(cb), turned(cc)


def fixed(a):
    return pltpu.with_memory_space_constraint(a, pltpu.HBM)


def turned(a):
    return jnp.transpose(a, (1, 0, 2))


def solution(mesh):
    NT = mesh.shape["tp"]
    NC = 8 if mesh.shape["ep"] >= 64 else 2
    NE = mesh.shape["ep"]
    ep = P("ep", None)
    in_specs = (
        ep, P("ep", "tp", None, None), P("ep", None, "tp"), P("ep", None, "tp"), P("ep", None, "tp"),
        P(None, "tp"), P(None, "tp"), P(None, "tp"), P(None, "tp"), P(), P("tp"), P("tp"), P("tp"),
        P(None, "tp"), P(None, "tp"), P(None, "tp"), P(), P("tp"), P("tp", None), P(), ep, ep,
        P("ep", None, "tp"), P("ep", None, "tp"), P("ep", "tp", None), P("ep", "tp"), P("ep", "tp"), P("tp", "ep"), P(),
    )
    out_specs = (P("ep", "tp"), P("ep", "tp", None, None), P("ep", None, "tp"), P("ep", None, "tp"), P("ep", None, "tp"))
    part = functools.partial(body, NE=NE, NC=NC, NT=NT, sd=128)
    return jax.shard_map(part, mesh=mesh, in_specs=in_specs, out_specs=out_specs, check_vma=False)
```

```python
import functools

import jax
import jax.numpy as jnp
from jax import lax
from jax.experimental import pallas as pl
from jax.experimental.pallas import tpu as pltpu
from jax.sharding import PartitionSpec as P

EPS = 1e-06
F32 = jnp.float32
BF16 = jnp.bfloat16
HIGH = lax.Precision.HIGHEST
MESH = pl.DeviceIdType.MESH
VMEM_STEP = 24_000_000
VMEM_STORE = 4_000_000


def dot(a, b, **kw):
    return jnp.dot(a, b, preferred_element_type=F32, **kw)


def dot_nt(a, b, **kw):
    return lax.dot_general(a, b, (((1,), (1,)), ((), ())), preferred_element_type=F32, **kw)


def iota(shape, dim):
    return lax.broadcasted_iota(jnp.int32, shape, dim)


def rms_rows(values, gain):
    return values * lax.rsqrt(jnp.mean(values * values, axis=-1, keepdims=True) + EPS) * gain


def silu(v):
    return v * jax.nn.sigmoid(v)


def step_kernel(NE, NC, NT, n_groups, *refs):
    given, refs = refs[:20], refs[20:]
    state, w_x, w_z, w_b, w_c, w_out, w_g, w_u, w_d = refs[:9]
    mixed, state_out, cx_out, cb_out, cc_out = refs[9:14]
    small, refs = refs[14:34], refs[34:]
    tokens, conv_x, conv_b, conv_c, w_dt, dt_bias, a_log, d_skip, taps_x, taps_b, taps_c, gain = small[:12]
    ggain, gain2, ids, wts, dgate, dup, ddown, bgate = small[12:]
    vx, vz, vb, vc, st, vo, vg, vu, vd, pt, d1, d2, d3, dq, tk, rt, bs_, br, aa, fs_, fx, fz, fr, gs_, gr, lsem, isem, tsem, ssem, rsem = refs
    NZ = NE // NC
    S, D = tokens.shape
    heads, hd, sd = st.shape[1:]
    inner = heads * hd
    per = heads // n_groups
    quarter = D // NT
    R = 2 * NE
    e = lax.axis_index("ep")
    t = lax.axis_index("tp")
    z = e // NC
    yc = lax.rem(e, NC)

    ts = [lax.rem(t + d, NT) for d in range(1, NT)]
    ring = sorted(range(NZ), key=lambda d: (min(d, NZ - d), d))
    half = NZ // 2
    groups = (ring[:half], ring[half:])
    at = [lax.rem(z + d, NZ) for d in range(NZ)]
    zs = [at[d] for d in reversed(ring) if d]
    around = [lax.rem(yc + d, NC) for d in range(NC)]
    cores = around[1:]
    barrier = pltpu.get_barrier_semaphore()
    for dev in [(p * NC + yc, t) for p in zs] + [(z * NC + p, t) for p in cores] + [(e, p) for p in ts]:
        pl.semaphore_signal(barrier, inc=1, device_id=dev, device_id_type=MESH)

    loads = {}
    for i, (name, src, dst) in enumerate((
        ("x", w_x, vx), ("b", w_b, vb), ("c", w_c, vc), ("z", w_z, vz), ("o", w_out, vo), ("d", w_d.at[0], vd), ("g", w_g.at[0], vg), ("u", w_u.at[0], vu)
    )):
        loads[name] = pltpu.make_async_copy(src, dst, lsem.at[i])
    tiny = [pltpu.make_async_copy(src, dst, tsem.at[i]) for i, (src, dst) in enumerate(zip(given, small))]
    for c in tiny[:12]:
        c.start()
    for name in "xbcz":
        loads[name].start()
    ins = [pltpu.make_async_copy(state.at[s], st.at[s], isem.at[s]) for s in range(S)]
    for c in ins:
        c.start()
    loads["o"].start()
    for c in tiny[12:]:
        c.start()
    for name in "dgu":
        loads[name].start()

    PART, ROUTE, DENSE, DENSE2, DOWN, TOK, SLOT, DOUT, HID, RET, TOK2, SLOT2, HID2, DZ = range(14)

    def send(i, src, dst, dev, there=None):
        pltpu.make_async_remote_copy(src_ref=src, dst_ref=dst, send_sem=ssem.at[i], recv_sem=rsem.at[i if there is None else there], device_id=dev, device_id_type=MESH).start()

    def wait(sem, ref, count):
        pltpu.make_async_copy(ref.at[pl.ds(0, count)], ref.at[pl.ds(0, count)], sem).wait()

    def arrive(i, ref, count):
        wait(rsem.at[i], ref, count)

    for c in tiny[:12]:
        c.wait()
    normed = rms_rows(tokens[...].astype(F32), gain[...]).astype(BF16)
    raw = dot_nt(normed, w_dt[...])
    total_heads = raw.shape[1]
    spread_all = (iota((total_heads, inner), 0) == t * heads + iota((total_heads, inner), 1) // hd).astype(F32)
    spread = (iota((heads, inner), 0) == iota((heads, inner), 1) // hd).astype(F32)
    raw = dot(raw, spread_all, precision=HIGH)
    bias = dot(dt_bias[...], spread, precision=HIGH)
    rate = jnp.exp(dot(a_log[...], spread, precision=HIGH))
    skip = dot(d_skip[...], spread, precision=HIGH)
    pre = raw + bias
    step = jnp.maximum(pre, 0.0) + jnp.log1p(jnp.exp(-jnp.abs(pre)))
    decay = jnp.exp(-step * rate)

    def conv(prev, fresh, taps, out):
        fresh = fresh.astype(BF16)
        tap = taps[...].astype(F32)
        depth = prev.shape[0]
        total = fresh.astype(F32) * tap[depth : depth + 1]
        for j in range(depth):
            total = total + prev[j].astype(F32) * tap[j : j + 1]
            out[j] = prev[j + 1] if j + 1 < depth else fresh
        return silu(total)

    for name in "xbc":
        loads[name].wait()
    xs = conv(conv_x, dot(normed, vx[...]), taps_x, cx_out)
    bs = conv(conv_b, dot(normed, vb[...]), taps_b, cb_out)
    cs = conv(conv_c, dot(normed, vc[...]), taps_c, cc_out)
    inflow = step * xs
    rows = per * hd
    loads["z"].wait()
    lane = iota((rows, S), 1)
    reads = [jnp.zeros((rows, S), F32) for _ in range(n_groups)]
    for s in range(S):
        if s % 4 == 0:
            for c in ins[s : s + 4]:
                c.wait()
        if s == 0:
            zz = dot(normed, vz[...]).astype(BF16).astype(F32)
        for g in range(n_groups):
            old = st[s, g * per : (g + 1) * per].reshape(rows, sd)
            got = jnp.sum(old * cs[s : s + 1, g * sd : (g + 1) * sd], axis=1, keepdims=True)
            reads[g] = jnp.where(lane == s, got, reads[g])
    both = [jnp.sum(bs[:, g * sd : (g + 1) * sd] * cs[:, g * sd : (g + 1) * sd], axis=1, keepdims=True) for g in range(n_groups)]
    for c in tiny[12:]:
        c.wait()
    parts = []
    for g in range(n_groups):
        cut = slice(g * rows, (g + 1) * rows)
        v = decay[:, cut] * reads[g].T + inflow[:, cut] * both[g] + skip[:, cut] * xs[:, cut]
        v = v * silu(zz[:, cut])
        parts.append(v * lax.rsqrt(jnp.mean(v * v, axis=-1, keepdims=True) + EPS) * ggain[:, cut])
    mixed_heads = jnp.concatenate(parts, axis=1).astype(BF16)
    loads["o"].wait()
    pt[t] = dot(mixed_heads, vo[...]).astype(BF16)

    pl.semaphore_wait(barrier, (NZ - 1) + (NC - 1) + (NT - 1))
    for p in ts:
        send(PART, pt.at[t], pt.at[t], (e, p))

    slot = iota((S, R), 1)
    named = jnp.zeros((S, R), F32)
    weight = jnp.zeros((S, R), F32)
    for k in range(ids.shape[1]):
        hit = ids[:, k : k + 1] == slot // 2
        named = jnp.where(hit, 1.0, named)
        weight = jnp.where(hit, wts[:, k : k + 1], weight)
    before = (iota((S, S), 0) > iota((S, S), 1)).astype(F32)
    rank = dot(before, named)
    mine = jnp.logical_and(named > 0.5, jnp.abs(rank - lax.rem(slot, 2).astype(F32)) < 0.5)
    rt[z] = jnp.where(mine, 1.0, 0.0).astype(BF16)
    give = jnp.where(mine, weight, 0.0)
    hs = dgate.shape[1] // NZ
    lane = iota((dgate.shape[0], 128), 1)
    three = [dgate[...].astype(F32), dup[...].astype(F32), ddown[...].astype(F32)]
    for k in range(NZ):
        page, off = k * hs // 128 * 128, k * hs % 128
        block = jnp.zeros(lane.shape, F32)
        for j, v in enumerate(three):
            v = v[:, page : page + 128]
            shift = (j * hs - off) % 128
            block = jnp.where(jnp.logical_and(lane >= j * hs, lane < (j + 1) * hs), pltpu.roll(v, shift, 1) if shift else v, block)
        d1[k] = block.astype(BF16)
    for p in zs:
        send(ROUTE, rt.at[z], rt.at[z], (p * NC + yc, t))
        send(DENSE, d1.at[p], d2.at[z], (p * NC + yc, t))
    d2[z] = d1[z]
    loads["d"].wait()

    in_col = inflow.T
    decay_col = decay.T
    for s in range(S):
        for g in range(n_groups):
            cut = slice(g * rows, (g + 1) * rows)
            old = st[s, g * per : (g + 1) * per].reshape(rows, sd)
            new = decay_col[cut, s : s + 1] * old + in_col[cut, s : s + 1] * bs[s : s + 1, g * sd : (g + 1) * sd]
            state_out[s, g * per : (g + 1) * per] = new.reshape(per, hd, sd)

    arrive(PART, pt, NT - 1)
    total = pt[0].astype(F32)
    for k in range(1, NT):
        total = total + pt[k].astype(F32)
    residual = (tokens[...].astype(F32) + total).astype(BF16).astype(F32)
    normed2 = rms_rows(residual, gain2[...]).astype(BF16)
    tk[z] = normed2
    for d in reversed(ring[1:]):
        send(TOK, tk.at[z], tk.at[z], (at[d] * NC + yc, t), TOK2 if (NZ - d) % NZ in groups[1] else TOK)

    for p in ts:
        send(DOWN, vd.at[:, pl.ds(pl.multiple_of(p * quarter, quarter), quarter)], dq.at[t], (e, p))
    dq[t] = vd[:, pl.ds(pl.multiple_of(t * quarter, quarter), quarter)]

    arrive(DENSE, d2, NZ - 1)
    for p in cores:
        send(DENSE2, d2, d3.at[:, yc], (z * NC + p, t))
    for k in range(NZ):
        d3[k, yc] = d2[k]

    lanes = bgate.shape[1]
    weighted = jnp.zeros((S, lanes), F32)
    for k in range(bgate.shape[0]):
        weighted = weighted + normed2[:, k * lanes : (k + 1) * lanes].astype(F32) * bgate[k : k + 1, :].astype(F32)
    branch = jax.nn.sigmoid(jnp.sum(weighted, axis=1, keepdims=True))
    own = jnp.zeros((S, quarter), F32)
    for k in range(NT):
        own = jnp.where(t == k, residual[:, k * quarter : (k + 1) * quarter], own)

    def stacked(ref, offsets):
        return jnp.concatenate([ref[at[d]].astype(F32) for d in offsets], axis=0).astype(BF16)

    arrive(ROUTE, rt, NZ - 1)
    rows_g = NC * half * 2
    row, col = iota((rows_g, R), 0), iota((rows_g, R), 1)
    pick = (col == z * 2 * NC + 2 * (row // (2 * half)) + lax.rem(row, 2)).astype(BF16)
    same = lax.rem(iota((rows_g, half * S), 0) // 2, half) == iota((rows_g, half * S), 1) // S
    takes = [jnp.where(same, dot_nt(pick, stacked(rt, group)), 0.0).astype(BF16) for group in groups]

    toks = []
    for k, group in enumerate(groups):
        arrive((TOK, TOK2)[k], tk, len(group) - (k == 0))
        toks.append(stacked(tk, group))
        bs_[k] = dot(takes[k], toks[k]).astype(BF16).reshape(bs_.shape[1:])
        for p in cores:
            send((SLOT, SLOT2)[k], bs_.at[k, p], br.at[k, yc], (z * NC + p, t))
        br[k, yc] = bs_[k, yc]

    arrive(DENSE2, d3, NZ * (NC - 1) // NC)
    dense_w = d3[...].reshape(D, 128)
    pre = dot(jnp.concatenate(toks, axis=0), dense_w)
    act = silu(pltpu.roll(pre, 2 * hs, 1)) * pltpu.roll(pre, hs, 1)
    lane = iota(act.shape, 1)
    act = jnp.where(jnp.logical_and(lane >= 2 * hs, lane < 3 * hs), act, 0.0).astype(BF16)
    out = dot_nt(act, dense_w)
    for k in range(NZ):
        for j in range(NT):
            fs_[j, k] = out[k * S : (k + 1) * S, j * quarter : (j + 1) * quarter].astype(BF16)
    for p in ts:
        send(DOUT, fs_.at[p], fx.at[t], (e, p))
    fx[t] = fs_[t]

    loads["g"].wait()
    loads["u"].wait()
    for k in range(2):
        arrive((SLOT, SLOT2)[k], br.at[k], NC - 1)
        arrived = br[k].reshape(rows_g, D)
        aa[k, t] = (silu(dot(arrived, vg[...])) * dot(arrived, vu[...])).astype(BF16)
        for p in ts:
            send((HID, HID2)[k], aa.at[k, t], aa.at[k, t], (e, p))

    arrive(DOUT, fx, NT - 1)
    for k in range(NZ):
        v = fx[0, k].astype(F32)
        for j in range(1, NT):
            v = v + fx[j, k].astype(F32)
        fz[k] = v.astype(BF16)
    for k in reversed(range(1, NZ)):
        send(DZ, fz.at[k], fr.at[z], (at[ring[k]] * NC + yc, t))
    fr[z] = fz[0]

    arrive(DOWN, dq, NT - 1)
    down = jnp.concatenate([dq[k] for k in range(NT)], axis=0)
    for k, group in enumerate(groups):
        arrive((HID, HID2)[k], aa.at[k], NT - 1)
        hidden = jnp.concatenate([aa[k, j] for j in range(NT)], axis=1)
        gs_[k] = dot(hidden, down).astype(BF16).reshape(gs_.shape[1:])
        for i in reversed(range(half)):

            for j in range(0 if group[i] else 1, NC):
                send(RET, gs_.at[k, around[j] * half + i], gr.at[e], (at[group[i]] * NC + around[j], t))
    gr[e] = gs_[0, yc * half]

    arrive(DZ, fr, NZ - 1)
    dense = jnp.zeros((S, quarter), F32)
    for k in range(NZ):
        dense = dense + fr[k].astype(F32)
    base = own + branch * dense
    arrive(RET, gr, NE - 1)
    mixed[...] = (base + dot(give.astype(BF16), gr[...].reshape(R, quarter))).astype(BF16)

    for i, ref, count in ((PART, pt, NT - 1), (ROUTE, rt, NZ - 1), (DENSE, d1, NZ - 1), (DENSE2, d3, NZ * (NC - 1) // NC), (DOWN, dq, NT - 1), (TOK, tk, NZ - 1), (SLOT, bs_.at[0], NC - 1), (SLOT2, bs_.at[1], NC - 1), (HID, aa.at[0], NT - 1), (HID2, aa.at[1], NT - 1), (RET, gr, NE - 1)):
        wait(ssem.at[i], ref, count)
    wait(ssem.at[DOUT], fx, NT - 1)
    wait(ssem.at[DZ], fr, NZ - 1)


def store_kernel(count, *refs):
    ins, outs, sem = refs[:count], refs[count : 2 * count], refs[2 * count]
    copies = [pltpu.make_async_copy(a, b, sem.at[i]) for i, (a, b) in enumerate(zip(ins, outs))]
    for c in copies:
        c.start()
    for c in copies:
        c.wait()


def body(
    tokens, ssm_state, conv_x, conv_b, conv_c, w_x, w_z, w_b, w_c, w_dt, dt_bias, a_log, d_skip, taps_x, taps_b, taps_c,
    norm1_gain, group_gain, w_out, norm2_gain, route_ids, route_weights, exp_gate, exp_up, exp_down, dense_gate, dense_up, dense_down, branch_gate,
    *, NE, NC, NT, sd,
):
    S, D = tokens.shape
    NZ = NE // NC
    inner = w_x.shape[1]
    cols = w_b.shape[1]
    quarter = D // NT
    hidden = exp_gate.shape[2]
    R = 2 * NE
    rows = dense_gate.shape[0]
    vm, hbm, free = (pl.BlockSpec(memory_space=m) for m in (pltpu.VMEM, pltpu.HBM, pl.ANY))
    dma = pltpu.SemaphoreType.DMA
    half = lambda *shape: pltpu.VMEM(shape, BF16)
    shape = jax.ShapeDtypeStruct
    small = (
        tokens, turned(conv_x), turned(conv_b), turned(conv_c), w_dt.T, dt_bias[None], a_log[None], d_skip[None], taps_x, taps_b, taps_c, norm1_gain[None],
        group_gain[None], norm2_gain[None], route_ids, route_weights, dense_gate, dense_up, dense_down.T, branch_gate.reshape(D // 128, 128),
    )
    made = pl.pallas_call(
        functools.partial(step_kernel, NE, NC, NT, cols // sd),
        name="step",
        out_shape=(
            shape((S, quarter), BF16), shape(ssm_state.shape, F32), shape((3, S, inner), BF16), shape((3, S, cols), BF16), shape((3, S, cols), BF16),
        ),
        in_specs=[hbm] * 29,
        out_specs=(vm,) * 5,
        scratch_shapes=[pltpu.VMEM(a.shape, a.dtype) for a in small]
        + [
            half(D, inner), half(D, inner), half(D, cols), half(D, cols), pltpu.VMEM(ssm_state.shape, F32),
            half(inner, D), half(D, hidden), half(D, hidden), half(hidden, D),
            half(NT, S, D), half(NZ, rows, 128), half(NZ, rows, 128), half(NZ, NC, rows, 128), half(NT, hidden, quarter),
            half(NZ, S, D), half(NZ, S, R), half(2, NC, NZ, D), half(2, NC, NZ, D), half(2, NT, R // 2, hidden),
            half(NT, NZ, S, quarter), half(NT, NZ, S, quarter), half(NZ, S, quarter), half(NZ, S, quarter),
            half(2, NE // 2, 2, quarter), half(NE, 2, quarter),
            dma((8,)), dma((S,)), dma((20,)), dma((14,)), dma((14,)),
        ],
        compiler_params=pltpu.CompilerParams(collective_id=0, has_side_effects=True, vmem_limit_bytes=VMEM_STEP),
    )(
        *(fixed(a) for a in small),
        *(fixed(a) for a in (ssm_state, w_x, w_z, w_b, w_c, w_out, exp_gate, exp_up, exp_down)),
    )
    mixed, state_next, cx, cb, cc = pl.pallas_call(
        functools.partial(store_kernel, len(made)),
        name="store",
        out_shape=tuple(shape(a.shape, a.dtype) for a in made),
        in_specs=[free] * len(made),
        out_specs=(hbm,) * len(made),
        scratch_shapes=[dma((len(made),))],
        compiler_params=pltpu.CompilerParams(vmem_limit_bytes=VMEM_STORE),
    )(*made)
    return mixed, state_next, turned(cx), turned(cb), turned(cc)


def fixed(a):
    return pltpu.with_memory_space_constraint(a, pltpu.HBM)


def turned(a):
    return jnp.transpose(a, (1, 0, 2))


def solution(mesh):
    NT = mesh.shape["tp"]
    NC = 8 if mesh.shape["ep"] >= 64 else 2
    NE = mesh.shape["ep"]
    ep = P("ep", None)
    in_specs = (
        ep, P("ep", "tp", None, None), P("ep", None, "tp"), P("ep", None, "tp"), P("ep", None, "tp"),
        P(None, "tp"), P(None, "tp"), P(None, "tp"), P(None, "tp"), P(), P("tp"), P("tp"), P("tp"),
        P(None, "tp"), P(None, "tp"), P(None, "tp"), P(), P("tp"), P("tp", None), P(), ep, ep,
        P("ep", None, "tp"), P("ep", None, "tp"), P("ep", "tp", None), P("ep", "tp"), P("ep", "tp"), P("tp", "ep"), P(),
    )
    out_specs = (P("ep", "tp"), P("ep", "tp", None, None), P("ep", None, "tp"), P("ep", None, "tp"), P("ep", None, "tp"))
    part = functools.partial(body, NE=NE, NC=NC, NT=NT, sd=128)
    return jax.shard_map(part, mesh=mesh, in_specs=in_specs, out_specs=out_specs, check_vma=False)
```
